512 devices in a mesh: row: 16 (over y, x), col: 32 (over z, core).
Axes of the slice: x: 4, y: 4, z: 16, core: 2. Of those that a mesh axis runs over, the one named last changes fastest.
Arguments:
- mix_input: bfloat16 [4, 65536, 512], P(None, ('row', 'col')), may hold values from -6 to 6
- group_maps: bfloat16 [4, 128, 128], replicated, may hold values from -0.5 to 0.5
- out_map: bfloat16 [512, 2048], replicated, may hold values from -0.25 to 0.25
Outputs:
- mixed: bfloat16 [4, 65536, 2048], P(None, ('row', 'col'))
The draws below stay inside these ranges and needn't reach their ends.
All inputs are finite; a program needn't handle non-finite values.
Results may differ from the reference program's by a relative error of at most 0.011.
Values may be sent and summed in bfloat16 or wider, within the bound.
A program may use at most 64 MiB of HBM per device.

```python
import jax
import jax.numpy as jnp
from jax import lax

MODEL = 2048
GROUPS = 4
GROUP_CH = 128
SEQS = 4
CHANNELS = 512
LENGTH = 65536


def level_of(stream_key, shape, cuts, low, high):
    gain, own = 1.0, jax.random.fold_in(stream_key, 6)
    for axis_at, parts in cuts:
        heights = jnp.exp(jax.random.uniform(jax.random.fold_in(own, axis_at), (parts,), jnp.float32, low / len(cuts), high / len(cuts)))
        gain = gain * jnp.repeat(heights, shape[axis_at] // parts).reshape([-1 if axis == axis_at else 1 for axis in range(len(shape))])
    return gain


def centred(stream_key, dims, width, reach, shards=(), held_as=jnp.bfloat16):
    values = jax.random.normal(stream_key, dims, jnp.float32) * width
    if len(shards) > 0:
        values = level_of(stream_key, dims, shards, -0.22, 0.18) * values
    return jnp.clip(values, min=-reach, max=reach).astype(held_as)


def setup_inputs(seed: int = 0) -> dict:
    key_of = jax.random.split(jax.random.key(seed), 4)
    return {
        "mix_input": centred(key_of[0], (SEQS, LENGTH, CHANNELS), 1.0, 6.0, ((1, 512),)),
        "group_maps": centred(key_of[1], (GROUPS, GROUP_CH, GROUP_CH), GROUP_CH ** -0.5, 0.5),
        "out_map": centred(key_of[2], (CHANNELS, MODEL), CHANNELS ** -0.5, 0.25),
    }


def reference(mix_input, group_maps, out_map):
    def one_sequence(sequence):
        signal = sequence.astype(jnp.float32).reshape(LENGTH, GROUPS, GROUP_CH)
        spectrum = jnp.fft.fft2(signal, axes=(0, 2), norm="ortho").real.astype(jnp.float32)
        spectrum = spectrum.astype(jnp.bfloat16)
        grouped = jnp.einsum("pgj,gjl->pgl", spectrum.astype(jnp.float32), group_maps.astype(jnp.float32))
        grouped = grouped.astype(jnp.bfloat16).reshape(LENGTH, CHANNELS)
        return jnp.dot(grouped, out_map, preferred_element_type=jnp.float32).astype(jnp.bfloat16)

    return lax.map(one_sequence, mix_input)
```

```python
import functools
import math

import jax
import jax.numpy as jnp
import numpy as np
from jax import lax
from jax.experimental import pallas as pl
from jax.experimental.pallas import tpu as pltpu
from jax.sharding import PartitionSpec as P

MESH = pl.DeviceIdType.MESH
F32, BF16 = jnp.float32, jnp.bfloat16
LENGTH, WIDTH = 65536, 128


def lane_roll(x, shift):
    return pltpu.roll(x, shift % 128, 1)


def lanes(shape):
    return lax.broadcasted_iota(jnp.int32, shape, len(shape) - 1)


def real_fft(xs):
    n = len(xs)
    if n == 1:
        return [xs[0]], [None]
    m = n // 2
    pe, qe = real_fft(xs[0::2])
    po, qo = real_fft(xs[1::2])
    ps, qs = [None] * (m + 1), [None] * (m + 1)
    ps[0], ps[m] = pe[0] + po[0], pe[0] - po[0]
    for k in range(1, m // 2 + (m % 2)):
        c, s = math.cos(2 * math.pi * k / n), math.sin(2 * math.pi * k / n)
        tr = c * po[k] + s * qo[k]
        ti = c * qo[k] - s * po[k]
        ps[k], qs[k] = pe[k] + tr, qe[k] + ti
        ps[m - k], qs[m - k] = pe[k] - tr, ti - qe[k]
    if m % 2 == 0:
        ps[m // 2], qs[m // 2] = pe[m // 2], -po[m // 2]
    return ps, qs


def row_stage(blocks, cos1, sin1, h, roll):
    lane = lanes(blocks[0].shape)
    sgn = jnp.where(lane < 64, -1.0, 1.0).astype(F32)
    special = jnp.logical_and(lane % 32 == 0, h == 0)
    sp_re = jnp.logical_and(special, lane < 64)
    sp_im = jnp.logical_and(special, lane >= 64)
    ps, qs = real_fft(blocks)
    ys = [None] * 16
    ys[0], ys[8] = ps[0], ps[8]
    for d in range(1, 8):
        rolled = roll(qs[d], 64)
        turned = sgn * rolled
        ys[d] = jnp.where(sp_re, ps[d], jnp.where(sp_im, rolled, ps[d] + turned))
        ys[16 - d] = jnp.where(sp_re, roll(ps[d], 64), jnp.where(sp_im, -qs[d], ps[d] - turned))
    outs = [ys[0]]
    cc, ss = cos1, sin1
    for d in range(1, 16):
        outs.append(ys[d] * cc + roll(ys[d], 64) * ss)
        if d < 15:
            cc, ss = cc * cos1 - ss * sin1, ss * cos1 + cc * sin1
    return outs


def block_transpose(tiles, lane, roll):
    a0, a1, a2, a3 = tiles
    low = lane < 64
    b0, b2 = jnp.where(low, a0, roll(a2, 64)), jnp.where(low, roll(a0, 64), a2)
    b1, b3 = jnp.where(low, a1, roll(a3, 64)), jnp.where(low, roll(a1, 64), a3)
    even = (lane // 32) % 2 == 0
    return (
        jnp.where(even, b0, roll(b1, 32)),
        jnp.where(even, roll(b0, 96), b1),
        jnp.where(even, b2, roll(b3, 32)),
        jnp.where(even, roll(b2, 96), b3),
    )


def col_stage(blocks, cos1, sin1, z, h, roll):
    lane = lanes(blocks[0].shape)
    sgn = jnp.where(lane < 64, -1.0, 1.0).astype(F32)
    kappa = -sgn
    device = jnp.logical_and(h == 0, lax.rem(z, 8) == 0)
    special = jnp.logical_and(lane % 32 == 0, device)
    zero_mask = jnp.logical_and(lane >= 0, z == 0)
    ps, qs = real_fft(blocks)
    ws = [None] * 32
    ws[0], ws[16] = ps[0], ps[16]
    for e in range(1, 16):
        turned = sgn * roll(qs[e], 64)
        ws[e], ws[32 - e] = ps[e] + turned, ps[e] - turned
    rolled = [roll(w, 64) for w in ws]
    cc, ss = cos1, sin1
    plus, hs = [ws[0]], [kappa * ws[0]]
    for e in range(1, 33):
        v = (32 - e) % 32
        hs.append(kappa * (ws[v] * cc - rolled[v] * ss))
        if e < 32:
            plus.append(ws[e] * cc + rolled[e] * ss)
            cc, ss = cc * cos1 - ss * sin1, ss * cos1 + cc * sin1
    tiles = [[], []]
    for e in range(32):
        gp, gm = plus[e], jnp.where(zero_mask, hs[e], hs[e + 1])
        half = 0.5 * (gp - gm)
        tiles[0].append(jnp.where(special, gp - half, gp))
        tiles[1].append(jnp.where(special, kappa * roll(half, 64), gm))
    return [
        [block_transpose(tiles[sign][4 * group : 4 * group + 4], lane, roll) for group in range(8)]
        for sign in range(2)
    ]


@functools.cache
def tables():
    ch = np.arange(128)
    maps = np.zeros((2, 128, 2, 2, 2, 32))
    for h in range(2):
        for li in range(32):
            l = 32 * h + li
            re = np.cos(2 * np.pi * ((ch * l) % 128) / 128)
            im = -np.sin(2 * np.pi * ((ch * l) % 128) / 128) if l else np.cos(np.pi * ch)
            for ph in range(2):
                maps[ph, :, h, 0, ph, li] = re
                maps[ph, :, h, 1, ph, li] = im
    maps = maps.reshape(256, 256)
    lane = np.arange(128)
    ph = (lane // 32) % 2
    kap = np.where(lane < 64, 1.0, -1.0)
    pos = 64 * ph[None, :] + np.arange(64)[:, None]
    row_pos = np.stack([pos, pos + 128])
    row_tab = np.stack([np.cos(2 * np.pi * row_pos / LENGTH), kap * np.sin(2 * np.pi * row_pos / LENGTH)])
    zs = 2 * np.pi * np.arange(16) * 256 / LENGTH
    z_tab = np.stack([np.cos(zs), np.sin(zs)])
    col_tab = np.stack([np.cos(2 * np.pi * pos / 4096), kap * np.sin(2 * np.pi * pos / 4096)])
    f = (8 * np.arange(16)[None, :] + np.arange(8)[:, None]).reshape(128)
    full = np.arange(128)
    ang = 2 * np.pi * ((f[:, None] * full[None, :]) % 128) / 128
    last = np.concatenate([np.cos(ang), np.sin(ang)], axis=1) / math.sqrt(LENGTH * WIDTH)
    flip = np.zeros((2, 16, 16, 16, 16))
    for fh in range(16):
        for d in range(16):
            flip[0, fh, d, d, fh] = 1
            flip[1, fh, d, (16 - d) % 16, fh] = 1
    flip = flip.reshape(2, 256, 256)
    pick = np.zeros((128, 128))
    for l in range(64):
        pick[l, l] = 1
        pick[64 + l, 128 - l if l else 64] = 1
    return {
        "maps": maps.astype(BF16),
        "row": row_tab.astype(np.float32),
        "z": z_tab.astype(np.float32),
        "col": col_tab.astype(np.float32),
        "last": last.astype(BF16),
        "flip": flip.astype(BF16),
        "pick": pick.astype(BF16),
    }


def mix_kernel(
    x_ref, maps_ref, row_ref, z_ref, col_ref, last_ref, flip_ref, out_ref,
    t_buf, r_buf, v_buf, w_buf, k_buf, o_buf, i_buf, j_buf, l_buf, send_sem, recv_sem,
):
    row = lax.axis_index("row")
    col = lax.axis_index("col")
    z = col // 2
    h = col % 2
    me = 2 * row + h

    def rc_peer(step):
        peer = lax.rem(me + step, 32)
        return peer, (peer // 2, 2 * z + peer % 2)

    def z_peer(step):
        peer = lax.rem(z + step, 16)
        return peer, (row, 2 * peer + h)

    barrier = pltpu.get_barrier_semaphore()

    def greet_rc(step, carry):
        pl.semaphore_signal(barrier, inc=1, device_id=rc_peer(step)[1], device_id_type=MESH)
        return carry

    def greet_z(step, carry):
        pl.semaphore_signal(barrier, inc=1, device_id=z_peer(step)[1], device_id_type=MESH)
        return carry

    lax.fori_loop(1, 16, greet_z, 0)
    lax.fori_loop(1, 32, greet_rc, 0)

    for s in range(4):
        lhs = jnp.concatenate(
            [
                jnp.concatenate(
                    [x_ref[s, 0:64, 128 * g : 128 * g + 128], x_ref[s, 64:128, 128 * g : 128 * g + 128]], axis=1
                )
                for g in range(4)
            ],
            axis=0,
        )
        res = jnp.dot(lhs, maps_ref[...], preferred_element_type=F32).astype(BF16)
        for g in range(4):
            for half in range(2):
                t_buf[2 * (4 * s + g) + half] = res[64 * g : 64 * g + 64, 128 * half : 128 * half + 128]

    pl.semaphore_wait(barrier, 46)

    def exchange(phase, src, dst, count, peer_of, slot, order):
        def start(step, carry):
            peer, device = peer_of(step)
            pltpu.make_async_remote_copy(
                src_ref=src.at[peer], dst_ref=dst.at[slot], send_sem=send_sem.at[phase], recv_sem=recv_sem.at[phase],
                device_id=device, device_id_type=MESH,
            ).start()
            return carry

        if order is None:
            lax.fori_loop(1, count, start, 0)
        else:
            for step in order:
                start(step, 0)
        dst[slot] = src[slot]

    def finish(phase, src, dst, count):
        pltpu.make_async_copy(src.at[pl.ds(0, count - 1)], dst.at[pl.ds(0, count - 1)], recv_sem.at[phase]).wait()

    def drain(phase, src, dst, count):
        pltpu.make_async_copy(src.at[pl.ds(0, count - 1)], dst.at[pl.ds(0, count - 1)], send_sem.at[phase]).wait()

    far_first = [8, 7, 9, 6, 10, 5, 11, 4, 12, 3, 13, 2, 14, 1, 15]
    exchange(0, t_buf, r_buf, 32, rc_peer, me, None)
    finish(0, t_buf, r_buf, 32)

    zc, zs = z_ref[0, z], z_ref[1, z]

    def row_body(step, carry):
        pc, rows = step // 4, pl.ds(pl.multiple_of(16 * (step % 4), 16), 16)
        kap = jnp.where(lanes((16, 128)) < 64, 1.0, -1.0).astype(F32)
        base_c, base_s = row_ref[0, pc, rows, :], row_ref[1, pc, rows, :]
        cos1 = base_c * zc - base_s * (kap * zs)
        sin1 = base_s * zc + base_c * (kap * zs)
        blocks = [r_buf[2 * a + pc, rows, :].astype(F32) for a in range(16)]
        outs = row_stage(blocks, cos1, sin1, h, lane_roll)
        for d in range(16):
            v_buf[d, pc, rows, :] = outs[d].astype(BF16)
        return carry

    lax.fori_loop(0, 8, row_body, 0)
    exchange(1, v_buf, w_buf, 16, z_peer, z, far_first)
    finish(1, v_buf, w_buf, 16)

    def col_body(step, carry):
        rows = pl.ds(pl.multiple_of(16 * step, 16), 16)
        blocks = [w_buf[q // 2, q % 2, rows, :].astype(F32) for q in range(32)]
        res = col_stage(blocks, col_ref[0, rows, :], col_ref[1, rows, :], z, h, lane_roll)
        for sign in range(2):
            for group in range(8):
                for part in range(4):
                    k_buf[sign, group, part, rows, :] = res[sign][group][part].astype(BF16)
        return carry

    lax.fori_loop(0, 4, col_body, 0)

    for sign in range(2):
        for pair in range(4):
            rhs = jnp.concatenate([k_buf[sign, 2 * pair + i].reshape(256, 128) for i in range(2)], axis=1)
            res = jnp.dot(last_ref[...], rhs, preferred_element_type=F32).astype(BF16)
            for fl in range(8):
                for i in range(2):
                    o_buf[2 * fl + pair // 2, sign, pair % 2, i] = res[16 * fl : 16 * fl + 16, 128 * i : 128 * i + 128]

    exchange(2, o_buf, i_buf, 16, z_peer, z, far_first)
    finish(2, o_buf, i_buf, 16)

    for sign in range(2):
        rhs = jnp.concatenate([i_buf[:, sign, e3, e2].reshape(256, 128) for e3 in range(2) for e2 in range(2)], axis=1)
        res = jnp.dot(flip_ref[sign], rhs, preferred_element_type=F32).astype(BF16)
        for fh in range(16):
            for e3 in range(2):
                for e2 in range(2):
                    at = 128 * (2 * e3 + e2)
                    j_buf[2 * fh + e3, sign, e2] = res[16 * fh : 16 * fh + 16, at : at + 128]

    exchange(3, j_buf, l_buf, 32, rc_peer, me, None)
    finish(3, j_buf, l_buf, 32)
    out_ref[...] = l_buf[...]
    drain(0, t_buf, r_buf, 32)
    drain(1, v_buf, w_buf, 16)
    drain(2, o_buf, i_buf, 16)
    drain(3, j_buf, l_buf, 32)


def spectrum_rows(tiles, roll):
    lane = lanes(tiles[0].shape)
    d = lax.broadcasted_iota(jnp.int32, tiles[0].shape, 0)
    swap = jnp.logical_and(d >= 9, lane % 32 == 0)
    first, third = jnp.where(swap, tiles[2], tiles[0]), jnp.where(swap, tiles[0], tiles[2])
    return block_transpose((first, tiles[1], third, tiles[3]), lane, roll)


def out_kernel(l_ref, group_ref, pick_ref, map_ref, out_ref, spec_buf, chosen_buf):
    @pl.when(pl.program_id(0) == 0)
    def _():
        for g in range(4):
            chosen_buf[g] = jnp.dot(pick_ref[...], group_ref[g], preferred_element_type=F32).astype(BF16)

    grouped = []
    for g in range(4):
        for e2 in range(2):
            tiles = [l_ref[2 * g + hh, sign, e2].astype(F32) for sign in range(2) for hh in range(2)]
            for ein, tile in enumerate(spectrum_rows(tiles, lane_roll)):
                at = 16 * (4 * e2 + ein)
                spec_buf[g, at : at + 16, :] = tile.astype(BF16)
        grouped.append(jnp.dot(spec_buf[g], chosen_buf[g], preferred_element_type=F32).astype(BF16))
    out_ref[0] = jnp.dot(jnp.concatenate(grouped, axis=1), map_ref[...], preferred_element_type=F32).astype(BF16)


def per_device(mix_input, group_maps, out_map):
    tab = tables()
    vmem = pl.BlockSpec(memory_space=pltpu.VMEM)
    landed = pl.pallas_call(
        mix_kernel,
        out_shape=jax.ShapeDtypeStruct((32, 2, 2, 16, 128), BF16),
        in_specs=[vmem, vmem, vmem, pl.BlockSpec(memory_space=pltpu.SMEM), vmem, vmem, vmem],
        out_specs=vmem,
        scratch_shapes=[
            pltpu.VMEM((32, 64, 128), BF16),
            pltpu.VMEM((32, 64, 128), BF16),
            pltpu.VMEM((16, 2, 64, 128), BF16),
            pltpu.VMEM((16, 2, 64, 128), BF16),
            pltpu.VMEM((2, 8, 4, 64, 128), BF16),
            pltpu.VMEM((16, 2, 2, 2, 16, 128), BF16),
            pltpu.VMEM((16, 2, 2, 2, 16, 128), BF16),
            pltpu.VMEM((32, 2, 2, 16, 128), BF16),
            pltpu.VMEM((32, 2, 2, 16, 128), BF16),
            pltpu.SemaphoreType.DMA((4,)),
            pltpu.SemaphoreType.DMA((4,)),
        ],
        compiler_params=pltpu.CompilerParams(collective_id=0, has_side_effects=True, vmem_limit_bytes=32 * 2**20),
    )(mix_input, *(jnp.asarray(tab[name]) for name in ("maps", "row", "z", "col", "last", "flip")))
    return pl.pallas_call(
        out_kernel,
        grid=(4,),
        out_shape=jax.ShapeDtypeStruct((4, 128, out_map.shape[1]), BF16),
        in_specs=[
            pl.BlockSpec((8, 2, 2, 16, 128), lambda s: (s, 0, 0, 0, 0)),
            pl.BlockSpec((4, 128, 128), lambda s: (0, 0, 0)),
            pl.BlockSpec((128, 128), lambda s: (0, 0)),
            pl.BlockSpec(out_map.shape, lambda s: (0, 0)),
        ],
        out_specs=pl.BlockSpec((1, 128, out_map.shape[1]), lambda s: (s, 0, 0)),
        scratch_shapes=[pltpu.VMEM((4, 128, 128), BF16), pltpu.VMEM((4, 128, 128), BF16)],
    )(landed, group_maps, jnp.asarray(tab["pick"]), out_map)


def solution(mesh):
    return jax.shard_map(
        per_device,
        mesh=mesh,
        in_specs=(P(None, ("row", "col"), None), P(), P()),
        out_specs=P(None, ("row", "col"), None),
        check_vma=False,
    )
```

```python
import functools
import math

import jax
import jax.numpy as jnp
import numpy as np
from jax import lax
from jax.experimental import pallas as pl
from jax.experimental.pallas import tpu as pltpu
from jax.sharding import PartitionSpec as P

MESH = pl.DeviceIdType.MESH
F32, BF16 = jnp.float32, jnp.bfloat16
LENGTH, WIDTH = 65536, 128


def lane_roll(x, shift):
    return pltpu.roll(x, shift % 128, 1)


def lanes(shape):
    return lax.broadcasted_iota(jnp.int32, shape, len(shape) - 1)


def real_fft(xs):
    n = len(xs)
    if n == 1:
        return [xs[0]], [None]
    m = n // 2
    pe, qe = real_fft(xs[0::2])
    po, qo = real_fft(xs[1::2])
    ps, qs = [None] * (m + 1), [None] * (m + 1)
    ps[0], ps[m] = pe[0] + po[0], pe[0] - po[0]
    for k in range(1, m // 2 + (m % 2)):
        c, s = math.cos(2 * math.pi * k / n), math.sin(2 * math.pi * k / n)
        tr = c * po[k] + s * qo[k]
        ti = c * qo[k] - s * po[k]
        ps[k], qs[k] = pe[k] + tr, qe[k] + ti
        ps[m - k], qs[m - k] = pe[k] - tr, ti - qe[k]
    if m % 2 == 0:
        ps[m // 2], qs[m // 2] = pe[m // 2], -po[m // 2]
    return ps, qs


def row_stage(blocks, cos1, sin1, has_zero, roll):
    lane = lanes(blocks[0].shape)
    sgn = jnp.where(lane < 64, -1.0, 1.0).astype(F32)
    ps, qs = real_fft(blocks)
    ys = [None] * 16
    ys[0], ys[8] = ps[0], ps[8]
    if has_zero is not None:
        special = jnp.logical_and(lane % 16 == 0, has_zero)
        sp_re = jnp.logical_and(special, lane < 64)
        sp_im = jnp.logical_and(special, lane >= 64)
    for d in range(1, 8):
        rolled = roll(qs[d], 64)
        turned = sgn * rolled
        ys[d], ys[16 - d] = ps[d] + turned, ps[d] - turned
        if has_zero is not None:
            ys[d] = jnp.where(sp_re, ps[d], jnp.where(sp_im, rolled, ys[d]))
            ys[16 - d] = jnp.where(sp_re, roll(ps[d], 64), jnp.where(sp_im, -qs[d], ys[16 - d]))
    outs = [ys[0]]
    cc, ss = cos1, sin1
    for d in range(1, 16):
        outs.append(ys[d] * cc + roll(ys[d], 64) * ss)
        if d < 15:
            cc, ss = cc * cos1 - ss * sin1, ss * cos1 + cc * sin1
    return outs


def block_transpose(tiles, roll):
    tiles = list(tiles)
    block = lanes(tiles[0].shape) // 16
    for dist in (4, 2, 1):
        keep = (block // dist) % 2 == 0
        for i in range(8):
            if i & dist == 0:
                a, b = tiles[i], tiles[i + dist]
                tiles[i] = jnp.where(keep, a, roll(b, 16 * dist))
                tiles[i + dist] = jnp.where(keep, roll(a, 128 - 16 * dist), b)
    return tiles


def col_stage(blocks, cos1, sin1, z, has_zero, roll):
    lane = lanes(blocks[0].shape)
    sgn = jnp.where(lane < 64, -1.0, 1.0).astype(F32)
    kappa = -sgn
    zero_mask = jnp.logical_and(lane >= 0, z == 0)
    ps, qs = real_fft(blocks)
    ws = [None] * 32
    ws[0], ws[16] = ps[0], ps[16]
    for e in range(1, 16):
        turned = sgn * roll(qs[e], 64)
        ws[e], ws[32 - e] = ps[e] + turned, ps[e] - turned
    rolled = [roll(w, 64) for w in ws]
    cc, ss = cos1, sin1
    plus, hs = [ws[0]], [kappa * ws[0]]
    for e in range(1, 33):
        v = (32 - e) % 32
        hs.append(kappa * (ws[v] * cc - rolled[v] * ss))
        if e < 32:
            plus.append(ws[e] * cc + rolled[e] * ss)
            cc, ss = cc * cos1 - ss * sin1, ss * cos1 + cc * sin1
    tiles = [plus, [jnp.where(zero_mask, hs[e], hs[e + 1]) for e in range(32)]]
    if has_zero is not None:
        special = jnp.logical_and(lane % 16 == 0, jnp.logical_and(has_zero, lax.rem(z, 8) == 0))
        for e in range(32):
            gp, gm = tiles[0][e], tiles[1][e]
            half = 0.5 * (gp - gm)
            tiles[0][e] = jnp.where(special, gp - half, gp)
            tiles[1][e] = jnp.where(special, kappa * roll(half, 64), gm)
    return [[block_transpose(tiles[sign][8 * g : 8 * g + 8], roll) for g in range(4)] for sign in range(2)]


def spectrum_rows(tiles, has_zero, roll):
    tiles = list(tiles)
    if has_zero:
        d = lax.broadcasted_iota(jnp.int32, tiles[0].shape, 0)
        swap = jnp.logical_and(d >= 9, lanes(tiles[0].shape) % 16 == 0)
        for i in (0, 4):
            tiles[i], tiles[i + 2] = jnp.where(swap, tiles[i + 2], tiles[i]), jnp.where(swap, tiles[i], tiles[i + 2])
    return block_transpose(tiles, roll)


@functools.cache
def tables():
    ch = np.arange(128)
    maps = np.zeros((4, 128, 2, 2, 2, 4, 16))
    for c in range(2):
        for h in range(2):
            for li in range(16):
                l = 32 * h + 16 * c + li
                re = np.cos(2 * np.pi * ((ch * l) % 128) / 128)
                im = -np.sin(2 * np.pi * ((ch * l) % 128) / 128) if l else np.cos(np.pi * ch)
                for ph in range(4):
                    maps[ph, :, c, h, 0, ph, li] = re
                    maps[ph, :, c, h, 1, ph, li] = im
    lane = np.arange(128)
    kap = np.where(lane < 64, 1.0, -1.0)
    pos = 32 * ((lane // 16) % 4)[None, :] + np.arange(32)[:, None]
    row_pos = np.stack([pos, pos + 128])[None] + 256 * np.arange(16)[:, None, None, None]
    row_tab = np.stack([np.cos(2 * np.pi * row_pos / LENGTH), kap * np.sin(2 * np.pi * row_pos / LENGTH)], axis=1)
    col_tab = np.stack([np.cos(2 * np.pi * pos / 4096), kap * np.sin(2 * np.pi * pos / 4096)])
    f = (8 * np.arange(16)[None, :] + np.arange(8)[:, None]).reshape(128)
    ang = 2 * np.pi * ((f[:, None] * np.arange(128)[None, :]) % 128) / 128
    last = np.concatenate([np.cos(ang), np.sin(ang)], axis=1) / math.sqrt(LENGTH * WIDTH)
    flip = np.zeros((2, 16, 16, 16, 16))
    for fh in range(16):
        for d in range(16):
            flip[0, fh, d, d, fh] = 1
            flip[1, fh, d, (16 - d) % 16, fh] = 1
    pick = np.zeros((2, 2, 2, 16, 128))
    for c in range(2):
        for h in range(2):
            for li in range(16):
                l = 32 * h + 16 * c + li
                pick[c, 0, h, li, l] = 1
                pick[c, 1, h, li, 128 - l if l else 64] = 1
    return {
        "maps": maps.reshape(512, 512).astype(BF16),
        "row": row_tab.astype(np.float32),
        "col": col_tab.astype(np.float32),
        "last": last.astype(BF16),
        "flip": flip.reshape(2, 256, 256).astype(BF16),
        "pick": pick.reshape(128, 128).astype(BF16),
    }


FAR_FIRST = (8, 7, 9, 6, 10, 5, 11, 4, 12, 3, 13, 2, 14, 1, 15)


def mix_kernel(
    x_hbm, maps_hbm, row_hbm, col_hbm, last_hbm, flip_hbm, pick_hbm, group_hbm, out_map_hbm, out_ref,
    x_ref, maps_ref, row_ref, col_ref, last_ref, flip_ref, pick_ref, group_ref, out_map_ref,
    t_buf, r_buf, v_buf, w_buf, k_buf, o_buf, i_buf, j_buf, l_buf, fused_buf, spec_buf, acc_buf,
    load_sem, send_sem, recv_sem,
):
    row = lax.axis_index("row")
    col = lax.axis_index("col")
    z = col // 2
    h = col % 2
    me = 2 * row + h

    pairs = (
        (x_hbm, x_ref), (maps_hbm, maps_ref), (row_hbm.at[z], row_ref), (col_hbm, col_ref), (last_hbm, last_ref),
        (flip_hbm, flip_ref), (pick_hbm, pick_ref), (group_hbm, group_ref), (out_map_hbm, out_map_ref),
    )
    loads = [pltpu.make_async_copy(src, dst, load_sem.at[i]) for i, (src, dst) in enumerate(pairs)]
    for load in loads:
        load.start()

    def rc_peer(step):
        peer = lax.rem(me + step, 32)
        return peer, (peer // 2, 2 * z + peer % 2)

    def z_peer(step):
        peer = lax.rem(z + step, 16)
        return peer, (row, 2 * peer + h)

    barrier = pltpu.get_barrier_semaphore()

    def greet_rc(step, carry):
        pl.semaphore_signal(barrier, inc=1, device_id=rc_peer(step)[1], device_id_type=MESH)
        return carry

    def greet_z(step, carry):
        pl.semaphore_signal(barrier, inc=1, device_id=z_peer(step)[1], device_id_type=MESH)
        return carry

    lax.fori_loop(1, 16, greet_z, 0)
    lax.fori_loop(1, 32, greet_rc, 0)

    def exchange(phase, c, src, dst, count, peer_of, slot, order):
        def start(step, carry):
            peer, device = peer_of(step)
            pltpu.make_async_remote_copy(
                src_ref=src.at[c, peer], dst_ref=dst.at[c, slot], send_sem=send_sem.at[phase, c],
                recv_sem=recv_sem.at[phase, c], device_id=device, device_id_type=MESH,
            ).start()
            return carry

        if order is None:
            lax.fori_loop(1, count, start, 0)
        else:
            for step in order:
                start(step, 0)
        dst[c, slot] = src[c, slot]

    def wait_all(sem, buf, c, count):
        span = buf.at[c, pl.ds(0, count - 1)]
        pltpu.make_async_copy(span, span, sem).wait()

    def rc_in(c):
        for s in range(4):
            lhs = jnp.concatenate(
                [
                    jnp.concatenate(
                        [x_ref[s, 32 * ph : 32 * ph + 32, 128 * g : 128 * g + 128] for ph in range(4)], axis=1
                    )
                    for g in range(4)
                ],
                axis=0,
            )
            res = jnp.dot(lhs, maps_ref[:, 256 * c : 256 * c + 256], preferred_element_type=F32).astype(BF16)
            for g in range(4):
                for half in range(2):
                    t_buf[c, 2 * (4 * s + g) + half] = res[32 * g : 32 * g + 32, 128 * half : 128 * half + 128]

    def row_transform(c):
        def body(step, carry):
            pc, rows = step // 2, pl.ds(pl.multiple_of(16 * (step % 2), 16), 16)
            cos1, sin1 = row_ref[0, pc, rows, :], row_ref[1, pc, rows, :]
            blocks = [r_buf[c, 2 * a + pc, rows, :].astype(F32) for a in range(16)]
            outs = row_stage(blocks, cos1, sin1, h == 0 if c == 0 else None, lane_roll)
            for d in range(16):
                v_buf[c, d, pc, rows, :] = outs[d].astype(BF16)
            return carry

        lax.fori_loop(0, 4, body, 0)

    def col_transform(c):
        def body(step, carry):
            rows = pl.ds(pl.multiple_of(16 * step, 16), 16)
            blocks = [w_buf[c, q // 2, q % 2, rows, :].astype(F32) for q in range(32)]
            res = col_stage(
                blocks, col_ref[0, rows, :], col_ref[1, rows, :], z, h == 0 if c == 0 else None, lane_roll
            )
            for sign in range(2):
                for group in range(4):
                    for part in range(8):
                        k_buf[sign, group, part, rows, :] = res[sign][group][part].astype(BF16)
            return carry

        lax.fori_loop(0, 2, body, 0)
        for sign in range(2):
            for e4 in range(2):
                rhs = jnp.concatenate([k_buf[sign, 2 * e4 + e3].reshape(256, 128) for e3 in range(2)], axis=1)
                res = jnp.dot(last_ref[...], rhs, preferred_element_type=F32).astype(BF16)
                for fl in range(8):
                    for e3 in range(2):
                        o_buf[c, 2 * fl + e4, sign, e3] = res[16 * fl : 16 * fl + 16, 128 * e3 : 128 * e3 + 128]

    def flip_rows(c):
        for sign in range(2):
            rhs = jnp.concatenate([i_buf[c, :, sign, e3].reshape(256, 128) for e3 in range(2)], axis=1)
            res = jnp.dot(flip_ref[sign], rhs, preferred_element_type=F32).astype(BF16)
            for fh in range(16):
                for e3 in range(2):
                    j_buf[c, 2 * fh + e3, sign] = res[16 * fh : 16 * fh + 16, 128 * e3 : 128 * e3 + 128]

    def fuse_maps():
        for g in range(4):
            chosen = jnp.dot(pick_ref[...], group_ref[g], preferred_element_type=F32).astype(BF16)
            for n in range(4):
                at = pl.ds(512 * n, 512)
                res = jnp.dot(chosen, out_map_ref[128 * g : 128 * g + 128, at], preferred_element_type=F32).astype(BF16)
                for c in range(2):
                    fused_buf[c, 64 * g : 64 * g + 64, at] = res[64 * c : 64 * c + 64]

    def spectrum(c):
        def body(step, carry):
            s, half = step // 2, step % 2
            tiles = [
                l_buf[c, 4 * step + 2 * gg + hh, sign].astype(F32)
                for gg in range(2)
                for sign in range(2)
                for hh in range(2)
            ]
            for el, tile in enumerate(spectrum_rows(tiles, c == 0, lane_roll)):
                rows = pl.ds(pl.multiple_of(128 * s + 16 * el, 16), 16)
                spec_buf[half, rows, :] = tile.astype(BF16)
            return carry

        lax.fori_loop(0, 8, body, 0)

    def output(c):
        lhs = jnp.concatenate([spec_buf[0], spec_buf[1]], axis=1)

        def body(n, carry):
            at = pl.ds(pl.multiple_of(256 * n, 256), 256)
            res = jnp.dot(lhs, fused_buf[c, :, at], preferred_element_type=F32)
            if c == 0:
                acc_buf[:, at] = res
            else:
                total = (acc_buf[:, at] + res).astype(BF16)
                for s in range(4):
                    out_ref[s, :, at] = total[128 * s : 128 * s + 128]
            return carry

        lax.fori_loop(0, 8, body, 0)

    loads[0].wait()
    loads[1].wait()
    with jax.named_scope("rc_in0"):
        rc_in(0)
    with jax.named_scope("barrier"):
        pl.semaphore_wait(barrier, 46)
    exchange(0, 0, t_buf, r_buf, 32, rc_peer, me, None)
    with jax.named_scope("rc_in1"):
        rc_in(1)
    exchange(0, 1, t_buf, r_buf, 32, rc_peer, me, None)
    loads[2].wait()
    for c in range(2):
        with jax.named_scope("wait_rc_in"):
            wait_all(recv_sem.at[0, c], r_buf, c, 32)
        with jax.named_scope("row_transform"):
            row_transform(c)
        exchange(1, c, v_buf, w_buf, 16, z_peer, z, FAR_FIRST)
    for load in loads[3:]:
        load.wait()
    with jax.named_scope("fuse_maps"):
        fuse_maps()
    for c in range(2):
        with jax.named_scope("wait_z_in"):
            wait_all(recv_sem.at[1, c], w_buf, c, 16)
        with jax.named_scope("col_transform"):
            col_transform(c)
        exchange(2, c, o_buf, i_buf, 16, z_peer, z, FAR_FIRST)
    for c in range(2):
        with jax.named_scope("wait_z_out"):
            wait_all(recv_sem.at[2, c], i_buf, c, 16)
        with jax.named_scope("flip"):
            flip_rows(c)
        exchange(3, c, j_buf, l_buf, 32, rc_peer, me, None)
        with jax.named_scope("wait_rc_out"):
            wait_all(recv_sem.at[3, c], l_buf, c, 32)
        with jax.named_scope("spectrum"):
            spectrum(c)
        with jax.named_scope("output"):
            output(c)
    for c in range(2):
        wait_all(send_sem.at[0, c], t_buf, c, 32)
        wait_all(send_sem.at[1, c], v_buf, c, 16)
        wait_all(send_sem.at[2, c], o_buf, c, 16)
        wait_all(send_sem.at[3, c], j_buf, c, 32)


def per_device(mix_input, group_maps, out_map):
    tab = tables()
    arrays = [mix_input] + [jnp.asarray(tab[name]) for name in ("maps", "row", "col", "last", "flip", "pick")]
    arrays += [group_maps, out_map]
    hbm = pl.BlockSpec(memory_space=pltpu.HBM)
    small = [pltpu.VMEM(a.shape[1:] if i == 2 else a.shape, a.dtype) for i, a in enumerate(arrays)]
    return pl.pallas_call(
        mix_kernel,
        out_shape=jax.ShapeDtypeStruct((4, 128, out_map.shape[1]), BF16),
        in_specs=[hbm] * len(arrays),
        out_specs=pl.BlockSpec(memory_space=pltpu.VMEM),
        scratch_shapes=small
        + [
            pltpu.VMEM((2, 32, 32, 128), BF16),
            pltpu.VMEM((2, 32, 32, 128), BF16),
            pltpu.VMEM((2, 16, 2, 32, 128), BF16),
            pltpu.VMEM((2, 16, 2, 32, 128), BF16),
            pltpu.VMEM((2, 4, 8, 32, 128), BF16),
            pltpu.VMEM((2, 16, 2, 2, 16, 128), BF16),
            pltpu.VMEM((2, 16, 2, 2, 16, 128), BF16),
            pltpu.VMEM((2, 32, 2, 16, 128), BF16),
            pltpu.VMEM((2, 32, 2, 16, 128), BF16),
            pltpu.VMEM((2, 256, out_map.shape[1]), BF16),
            pltpu.VMEM((2, 512, 128), BF16),
            pltpu.VMEM((512, out_map.shape[1]), F32),
            pltpu.SemaphoreType.DMA((9,)),
            pltpu.SemaphoreType.DMA((4, 2)),
            pltpu.SemaphoreType.DMA((4, 2)),
        ],
        compiler_params=pltpu.CompilerParams(collective_id=0, has_side_effects=True, vmem_limit_bytes=64937984),
    )(*arrays)


def solution(mesh):
    return jax.shard_map(
        per_device,
        mesh=mesh,
        in_specs=(P(None, ("row", "col"), None), P(), P()),
        out_specs=P(None, ("row", "col"), None),
        check_vma=False,
    )
```

```python
import functools
import math

import jax
import jax.numpy as jnp
import numpy as np
from jax import lax
from jax.experimental import pallas as pl
from jax.experimental.pallas import tpu as pltpu
from jax.sharding import PartitionSpec as P

MESH = pl.DeviceIdType.MESH
F32, BF16 = jnp.float32, jnp.bfloat16
LENGTH, WIDTH = 65536, 128
FAR_FIRST = (8, 7, 9, 6, 10, 5, 11, 4, 12, 3, 13, 2, 14, 1, 15)


@functools.cache
def tables():
    ch = np.arange(128)
    chan = np.zeros((2, 2, 32, 128))
    pick = np.zeros((2, 2, 32, 128))
    for c in range(2):
        for lg in range(32):
            l = 32 * c + lg
            chan[c, 0, lg] = np.cos(2 * np.pi * ((ch * l) % 128) / 128)
            chan[c, 1, lg] = -np.sin(2 * np.pi * ((ch * l) % 128) / 128) if l else np.cos(np.pi * ch)
            if l:
                pick[c, 0, lg, [l, 128 - l]] = 1, 1
                pick[c, 1, lg, [l, 128 - l]] = -1, 1
            else:
                pick[c, 0, lg, 0] = pick[c, 1, lg, 64] = 1
    in_flip = np.zeros((16, 16, 16, 16))
    out_flip = np.zeros((8, 32, 32, 8))
    for i in range(16):
        for j in range(16):
            in_flip[i, j, j, i] = 1
    for i in range(8):
        for j in range(32):
            out_flip[i, j, j, i] = 1
    src = np.arange(512)
    q = 32 * (src // 32) + src // 16 % 2 + 2 * (src % 16)
    k1 = np.arange(512)
    ang = 2 * np.pi * ((k1[:, None] * q[None, :]) % 512) / 512
    turn = 2 * np.pi * k1[:, None] * np.arange(128)[None, :] / LENGTH
    fang = 2 * np.pi * ((np.arange(128)[:, None] * np.arange(128)[None, :]) % 128) / 128
    last = np.stack(
        [np.concatenate([np.cos(fang), np.sin(fang)], axis=1), np.concatenate([-np.sin(fang), np.cos(fang)], axis=1)]
    ) / math.sqrt(LENGTH * WIDTH)
    return {
        "chan": chan.reshape(128, 128).astype(BF16),
        "in_flip": in_flip.reshape(256, 256).astype(BF16),
        "dft": np.concatenate([np.cos(ang), -np.sin(ang)]).astype(BF16),
        "turn": np.stack([np.cos(turn), np.sin(turn)]).astype(np.float32),
        "last": last.astype(BF16),
        "out_flip": out_flip.reshape(256, 256).astype(BF16),
        "pick": pick.reshape(128, 128).astype(BF16),
    }


def mix_kernel(
    x_hbm, chan_hbm, in_flip_hbm, dft_hbm, turn_hbm, last_hbm, out_flip_hbm, pick_hbm, group_hbm, out_ref,
    x_ref, chan_ref, in_flip_ref, dft_ref, turn_ref, last_ref, out_flip_ref, pick_ref, group_ref,
    t_buf, w_buf, v_buf, r_buf, f_buf, g_buf, o_buf, m_buf, j_buf, s_buf, chosen_buf, load_sem, send_sem, recv_sem,
):
    row = lax.axis_index("row")
    col = lax.axis_index("col")
    z = col // 2
    h = col % 2
    me = 2 * row + h

    pairs = tuple((x_hbm.at[s], x_ref.at[s]) for s in range(4)) + (
        (chan_hbm, chan_ref), (in_flip_hbm, in_flip_ref), (dft_hbm, dft_ref), (turn_hbm, turn_ref),
        (last_hbm, last_ref), (out_flip_hbm, out_flip_ref), (pick_hbm, pick_ref), (group_hbm, group_ref),
    )
    loads = [pltpu.make_async_copy(src, dst, load_sem.at[i]) for i, (src, dst) in enumerate(pairs)]
    for load in loads[:5]:
        load.start()

    def rc_peer(step):
        peer = lax.rem(me + step, 32)
        return peer, (peer // 2, 2 * z + peer % 2)

    def z_peer(step):
        peer = lax.rem(z + step, 16)
        return peer, (row, 2 * peer + h)

    barrier = pltpu.get_barrier_semaphore()

    for step in range(1, 16):
        pl.semaphore_signal(barrier, inc=1, device_id=z_peer(step)[1], device_id_type=MESH)
    for step in range(1, 32):
        pl.semaphore_signal(barrier, inc=1, device_id=rc_peer(step)[1], device_id_type=MESH)

    def exchange(phase, c, src, dst, peer_of, slot, order):
        for step in order:
            peer, device = peer_of(step)
            pltpu.make_async_remote_copy(
                src_ref=src.at[c, peer], dst_ref=dst.at[c, slot], send_sem=send_sem.at[phase, c],
                recv_sem=recv_sem.at[phase, c], device_id=device, device_id_type=MESH,
            ).start()
        dst[c, slot] = src[c, slot]

    def wait_all(sem, buf, c, count):
        span = buf.at[c, pl.ds(0, count - 1)]
        pltpu.make_async_copy(span, span, sem).wait()

    def channel_transform():
        for g in range(4):
            rhs = jnp.concatenate([x_ref[s, :, 128 * g : 128 * g + 128] for s in range(4)], axis=0)
            res = lax.dot_general(chan_ref[...], rhs, (((1,), (1,)), ((), ())), preferred_element_type=F32)
            res = res.astype(BF16)
            for c in range(4):
                for s in range(4):
                    t_buf[c, 4 * s + g] = res[32 * c : 32 * c + 32, 128 * s : 128 * s + 128]

    def in_turn(c):
        rhs = jnp.concatenate([w_buf[c, :, 16 * b : 16 * b + 16, :].reshape(256, 128) for b in range(2)], axis=1)
        res = jnp.dot(in_flip_ref[...], rhs, preferred_element_type=F32).astype(BF16)
        for b in range(2):
            for i in range(16):
                v_buf[c, 16 * b + i] = res[16 * i : 16 * i + 16, 128 * b : 128 * b + 128]

    def transform(c):
        f_buf[...] = jnp.dot(dft_ref[...], r_buf[c].reshape(512, 128), preferred_element_type=F32)

        def body(step, carry):
            rows = pl.ds(pl.multiple_of(64 * step, 64), 64)
            under = pl.ds(pl.multiple_of(512 + 64 * step, 64), 64)
            re, im, cos, sin = f_buf[rows, :], f_buf[under, :], turn_ref[0, rows, :], turn_ref[1, rows, :]
            g_buf[rows, 0:128] = (re * cos + im * sin).astype(BF16)
            g_buf[rows, 128:256] = (im * cos - re * sin).astype(BF16)
            return carry

        lax.fori_loop(0, 8, body, 0)
        kind = jnp.where(me == 0, 0, 1) if c == 1 else c % 2
        res = lax.dot_general(
            last_ref[kind], g_buf[...], (((1,), (1,)), ((), ())), preferred_element_type=F32
        ).astype(BF16)
        for fh in range(16):
            for e3 in range(2):
                for e4 in range(2):
                    at = 256 * e4 + 128 * e3
                    o_buf[c, 2 * fh + e3, e4] = res[8 * fh : 8 * fh + 8, at : at + 128]

    def out_turn(c):
        rhs = jnp.concatenate([m_buf[c, :, e4].reshape(256, 128) for e4 in range(2)], axis=1)
        res = jnp.dot(out_flip_ref[...], rhs, preferred_element_type=F32).astype(BF16)
        for fl in range(8):
            for e4 in range(2):
                j_buf[c, 2 * fl + e4] = res[32 * fl : 32 * fl + 32, 128 * e4 : 128 * e4 + 128]

    def choose():
        for g in range(4):
            chosen_buf[g] = jnp.dot(pick_ref[...], group_ref[g], preferred_element_type=F32).astype(BF16)

    def group():
        for g in range(4):
            lhs = jnp.concatenate(
                [
                    jnp.concatenate([s_buf[c, 4 * s + g] for c in range(4)], axis=0)
                    for s in range(4)
                ],
                axis=1,
            )
            res = lax.dot_general(lhs, chosen_buf[g], (((0,), (0,)), ((), ())), preferred_element_type=F32)
            out_ref[:, 128 * g : 128 * g + 128] = res.astype(BF16)

    def scope(name, run, *args):
        with jax.named_scope(name):
            run(*args)

    for load in loads[:5]:
        load.wait()
    scope("channel", channel_transform)
    with jax.named_scope("barrier"):
        pl.semaphore_wait(barrier, 46)
    for c in range(4):
        exchange(0, c, t_buf, w_buf, z_peer, z, FAR_FIRST)
    for load in loads[5:]:
        load.start()
    for load in loads[5:]:
        load.wait()
    scope("choose", choose)

    def z_in(c):
        scope(f"wait_z_in{c}", wait_all, recv_sem.at[0, c], w_buf, c, 16)
        scope(f"in_turn{c}", in_turn, c)
        exchange(1, c, v_buf, r_buf, rc_peer, me, range(1, 32))

    def rc_in(c):
        scope(f"wait_rc_in{c}", wait_all, recv_sem.at[1, c], r_buf, c, 32)
        scope(f"transform{c}", transform, c)
        exchange(2, c, o_buf, m_buf, rc_peer, me, range(1, 32))

    def rc_out(c):
        scope(f"wait_rc_out{c}", wait_all, recv_sem.at[2, c], m_buf, c, 32)
        scope(f"out_turn{c}", out_turn, c)
        exchange(3, c, j_buf, s_buf, z_peer, z, FAR_FIRST)

    order = (
        (z_in, 0), (z_in, 1), (rc_in, 0), (z_in, 2), (rc_in, 1), (rc_out, 0), (z_in, 3), (rc_in, 2), (rc_out, 1),
        (rc_in, 3), (rc_out, 2), (rc_out, 3),
    )
    for stage, c in order:
        stage(c)
    for c in range(4):
        wait_all(send_sem.at[0, c], t_buf, c, 16)
        wait_all(send_sem.at[1, c], v_buf, c, 32)
        wait_all(send_sem.at[2, c], o_buf, c, 32)
    for c in range(4):
        scope(f"wait_z_out{c}", wait_all, recv_sem.at[3, c], s_buf, c, 16)
    scope("group", group)
    for c in range(4):
        wait_all(send_sem.at[3, c], j_buf, c, 16)


def per_device(mix_input, group_maps, out_map):
    tab = tables()
    names = ("chan", "in_flip", "dft", "turn", "last", "out_flip", "pick")
    arrays = [mix_input] + [jnp.asarray(tab[name]) for name in names] + [group_maps]
    hbm = pl.BlockSpec(memory_space=pltpu.HBM)
    grouped = pl.pallas_call(
        mix_kernel,
        out_shape=jax.ShapeDtypeStruct((512, 512), BF16),
        in_specs=[hbm] * len(arrays),
        out_specs=pl.BlockSpec(memory_space=pltpu.VMEM),
        scratch_shapes=[pltpu.VMEM(a.shape, a.dtype) for a in arrays]
        + [
            pltpu.VMEM((4, 16, 32, 128), BF16),
            pltpu.VMEM((4, 16, 32, 128), BF16),
            pltpu.VMEM((4, 32, 16, 128), BF16),
            pltpu.VMEM((4, 32, 16, 128), BF16),
            pltpu.VMEM((1024, 128), F32),
            pltpu.VMEM((512, 256), BF16),
            pltpu.VMEM((4, 32, 2, 8, 128), BF16),
            pltpu.VMEM((4, 32, 2, 8, 128), BF16),
            pltpu.VMEM((4, 16, 32, 128), BF16),
            pltpu.VMEM((4, 16, 32, 128), BF16),
            pltpu.VMEM((4, 128, 128), BF16),
            pltpu.SemaphoreType.DMA((12,)),
            pltpu.SemaphoreType.DMA((4, 4)),
            pltpu.SemaphoreType.DMA((4, 4)),
        ],
        compiler_params=pltpu.CompilerParams(collective_id=0, has_side_effects=True, vmem_limit_bytes=64937984),
    )(*arrays)
    mixed = jnp.dot(grouped, out_map, preferred_element_type=F32).astype(BF16)
    return mixed.reshape(4, 128, out_map.shape[1])


def solution(mesh):
    return jax.shard_map(
        per_device,
        mesh=mesh,
        in_specs=(P(None, ("row", "col"), None), P(), P()),
        out_specs=P(None, ("row", "col"), None),
        check_vma=False,
    )
```

```python
import functools
import math

import jax
import jax.numpy as jnp
import numpy as np
from jax import lax
from jax.experimental import pallas as pl
from jax.experimental.pallas import tpu as pltpu
from jax.sharding import PartitionSpec as P

MESH = pl.DeviceIdType.MESH
F32, BF16 = jnp.float32, jnp.bfloat16
LENGTH, WIDTH = 65536, 128
FAR_FIRST = (8, 7, 9, 6, 10, 5, 11, 4, 12, 3, 13, 2, 14, 1, 15)


@functools.cache
def tables():
    ch = np.arange(128)
    chan = np.zeros((2, 2, 32, 128))
    pick = np.zeros((2, 2, 32, 128))
    for c in range(2):
        for lg in range(32):
            l = 32 * c + lg
            chan[c, 0, lg] = np.cos(2 * np.pi * ((ch * l) % 128) / 128)
            chan[c, 1, lg] = -np.sin(2 * np.pi * ((ch * l) % 128) / 128) if l else np.cos(np.pi * ch)
            if l:
                pick[c, 0, lg, [l, 128 - l]] = 1, 1
                pick[c, 1, lg, [l, 128 - l]] = -1, 1
            else:
                pick[c, 0, lg, 0] = pick[c, 1, lg, 64] = 1
    in_flip = np.zeros((16, 16, 16, 16))
    out_flip = np.zeros((8, 32, 32, 8))
    for i in range(16):
        for j in range(16):
            in_flip[i, j, j, i] = 1
    for i in range(8):
        for j in range(32):
            out_flip[i, j, j, i] = 1
    src = np.arange(512)
    q = 32 * (src // 32) + src // 16 % 2 + 2 * (src % 16)
    k1 = np.arange(512)
    ang = 2 * np.pi * ((k1[:, None] * q[None, :]) % 512) / 512
    turn = 2 * np.pi * k1[:, None] * np.arange(128)[None, :] / LENGTH
    fang = 2 * np.pi * ((np.arange(128)[:, None] * np.arange(128)[None, :]) % 128) / 128
    last = np.stack(
        [np.concatenate([np.cos(fang), np.sin(fang)], axis=1), np.concatenate([-np.sin(fang), np.cos(fang)], axis=1)]
    ) / math.sqrt(LENGTH * WIDTH)
    return {
        "chan": chan.reshape(128, 128).astype(BF16),
        "in_flip": in_flip.reshape(256, 256).astype(BF16),
        "dft": np.concatenate([np.cos(ang), -np.sin(ang)]).astype(BF16),
        "turn": np.stack([np.cos(turn), np.sin(turn)]).astype(np.float32),
        "last": last.astype(BF16),
        "out_flip": out_flip.reshape(256, 256).astype(BF16),
        "pick": pick.reshape(128, 128).astype(BF16),
    }


def mix_kernel(
    x_hbm, chan_hbm, in_flip_hbm, dft_hbm, turn_hbm, last_hbm, out_flip_hbm, pick_hbm, group_hbm, out_map_hbm,
    rows_ref, part_ref, late_map_ref, x_ref, chan_ref, in_flip_ref, dft_ref, turn_ref, last_ref, out_flip_ref, pick_ref, group_ref, out_map_ref,
    t_buf, w_buf, v_buf, r_buf, f_buf, g_buf, o_buf, m_buf, j_buf, s_buf, fused_buf, acc_buf, load_sem, send_sem, recv_sem,
):
    row = lax.axis_index("row")
    col = lax.axis_index("col")
    z = col // 2
    h = col % 2
    me = 2 * row + h

    pairs = tuple((x_hbm.at[s], x_ref.at[s]) for s in range(4)) + (
        (chan_hbm, chan_ref), (in_flip_hbm, in_flip_ref), (dft_hbm, dft_ref), (turn_hbm, turn_ref),
        (last_hbm, last_ref), (out_flip_hbm, out_flip_ref), (pick_hbm, pick_ref), (group_hbm, group_ref),
        (out_map_hbm, out_map_ref),
    )
    loads = [pltpu.make_async_copy(src, dst, load_sem.at[i]) for i, (src, dst) in enumerate(pairs)]
    for load in loads[:5]:
        load.start()

    def rc_peer(step):
        peer = lax.rem(me + step, 32)
        return peer, (peer // 2, 2 * z + peer % 2)

    def z_peer(step):
        peer = lax.rem(z + step, 16)
        return peer, (row, 2 * peer + h)

    barrier = pltpu.get_barrier_semaphore()

    for step in range(1, 16):
        pl.semaphore_signal(barrier, inc=1, device_id=z_peer(step)[1], device_id_type=MESH)
    for step in range(1, 32):
        pl.semaphore_signal(barrier, inc=1, device_id=rc_peer(step)[1], device_id_type=MESH)

    def exchange(phase, c, src, dst, peer_of, slot, order):
        for step in order:
            peer, device = peer_of(step)
            pltpu.make_async_remote_copy(
                src_ref=src.at[c, peer], dst_ref=dst.at[c, slot], send_sem=send_sem.at[phase, c],
                recv_sem=recv_sem.at[phase, c], device_id=device, device_id_type=MESH,
            ).start()
        dst[c, slot] = src[c, slot]

    def wait_all(sem, buf, c, count):
        span = buf.at[c, pl.ds(0, count - 1)]
        pltpu.make_async_copy(span, span, sem).wait()

    def channel_transform():
        for g in range(4):
            rhs = jnp.concatenate([x_ref[s, :, 128 * g : 128 * g + 128] for s in range(4)], axis=0)
            res = lax.dot_general(chan_ref[...], rhs, (((1,), (1,)), ((), ())), preferred_element_type=F32)
            res = res.astype(BF16)
            for c in range(4):
                for s in range(4):
                    t_buf[c, 4 * s + g] = res[32 * c : 32 * c + 32, 128 * s : 128 * s + 128]

    def in_turn(c):
        rhs = jnp.concatenate([w_buf[c, :, 16 * b : 16 * b + 16, :].reshape(256, 128) for b in range(2)], axis=1)
        res = jnp.dot(in_flip_ref[...], rhs, preferred_element_type=F32).astype(BF16)
        for b in range(2):
            for i in range(16):
                v_buf[c, 16 * b + i] = res[16 * i : 16 * i + 16, 128 * b : 128 * b + 128]

    def transform(c):
        f_buf[...] = jnp.dot(dft_ref[...], r_buf[c].reshape(512, 128), preferred_element_type=F32)

        def body(step, carry):
            rows = pl.ds(pl.multiple_of(64 * step, 64), 64)
            under = pl.ds(pl.multiple_of(512 + 64 * step, 64), 64)
            re, im, cos, sin = f_buf[rows, :], f_buf[under, :], turn_ref[0, rows, :], turn_ref[1, rows, :]
            g_buf[rows, 0:128] = (re * cos + im * sin).astype(BF16)
            g_buf[rows, 128:256] = (im * cos - re * sin).astype(BF16)
            return carry

        lax.fori_loop(0, 8, body, 0)
        kind = jnp.where(me == 0, 0, 1) if c == 1 else c % 2
        res = lax.dot_general(
            last_ref[kind], g_buf[...], (((1,), (1,)), ((), ())), preferred_element_type=F32
        ).astype(BF16)
        for fh in range(16):
            for e3 in range(2):
                for e4 in range(2):
                    at = 256 * e4 + 128 * e3
                    o_buf[c, 2 * fh + e3, e4] = res[8 * fh : 8 * fh + 8, at : at + 128]

    def out_turn(c):
        rhs = jnp.concatenate([m_buf[c, :, e4].reshape(256, 128) for e4 in range(2)], axis=1)
        res = jnp.dot(out_flip_ref[...], rhs, preferred_element_type=F32).astype(BF16)
        for fl in range(8):
            for e4 in range(2):
                j_buf[c, 2 * fl + e4] = res[32 * fl : 32 * fl + 32, 128 * e4 : 128 * e4 + 128]

    def fuse_maps():
        for g in range(4):
            chosen = jnp.dot(pick_ref[...], group_ref[g], preferred_element_type=F32).astype(BF16)
            for n in range(4):
                at = pl.ds(512 * n, 512)
                res = jnp.dot(chosen, out_map_ref[128 * g : 128 * g + 128, at], preferred_element_type=F32).astype(BF16)
                for c in range(3):
                    fused_buf[c, 32 * g : 32 * g + 32, at] = res[32 * c : 32 * c + 32]
                late_map_ref[32 * g : 32 * g + 32, at] = res[96:128]

    def spectrum_rows(c):
        return jnp.concatenate([s_buf[c, 4 * s : 4 * s + 4].reshape(128, 128).T for s in range(4)], axis=0)

    def first_product():
        lhs = jnp.concatenate([spectrum_rows(0), spectrum_rows(1)], axis=1)

        def body(n, carry):
            at = pl.ds(pl.multiple_of(256 * n, 256), 256)
            acc_buf[:, at] = jnp.dot(lhs, fused_buf[0:2, :, at].reshape(256, 256), preferred_element_type=F32)
            return carry

        lax.fori_loop(0, 8, body, 0)

    def second_product():
        lhs = spectrum_rows(2)

        def body(n, carry):
            at = pl.ds(pl.multiple_of(256 * n, 256), 256)
            res = jnp.dot(lhs, fused_buf[2, :, at], preferred_element_type=F32)
            part_ref[:, at] = (acc_buf[:, at] + res).astype(BF16)
            return carry

        lax.fori_loop(0, 8, body, 0)

    def last_rows():
        rows_ref[...] = spectrum_rows(3)

    def scope(name, run, *args):
        with jax.named_scope(name):
            run(*args)

    for load in loads[:5]:
        load.wait()
    scope("channel", channel_transform)
    with jax.named_scope("barrier"):
        pl.semaphore_wait(barrier, 46)
    for c in range(4):
        exchange(0, c, t_buf, w_buf, z_peer, z, FAR_FIRST)
    for load in loads[5:]:
        load.start()
    for load in loads[5:]:
        load.wait()
    scope("fuse_maps", fuse_maps)

    def z_in(c):
        scope(f"wait_z_in{c}", wait_all, recv_sem.at[0, c], w_buf, c, 16)
        scope(f"in_turn{c}", in_turn, c)
        exchange(1, c, v_buf, r_buf, rc_peer, me, range(1, 32))

    def rc_in(c):
        scope(f"wait_rc_in{c}", wait_all, recv_sem.at[1, c], r_buf, c, 32)
        scope(f"transform{c}", transform, c)
        exchange(2, c, o_buf, m_buf, rc_peer, me, range(1, 32))

    def rc_out(c):
        scope(f"wait_rc_out{c}", wait_all, recv_sem.at[2, c], m_buf, c, 32)
        scope(f"out_turn{c}", out_turn, c)
        exchange(3, c, j_buf, s_buf, z_peer, z, FAR_FIRST)

    order = (
        (z_in, 0), (z_in, 1), (rc_in, 0), (z_in, 2), (rc_in, 1), (rc_out, 0), (z_in, 3), (rc_in, 2), (rc_out, 1),
        (rc_in, 3), (rc_out, 2), (rc_out, 3),
    )
    for stage, c in order:
        stage(c)
    for c in range(2):
        scope(f"wait_z_out{c}", wait_all, recv_sem.at[3, c], s_buf, c, 16)
    scope("first_product", first_product)
    scope("wait_z_out2", wait_all, recv_sem.at[3, 2], s_buf, 2, 16)
    scope("second_product", second_product)
    for c in range(4):
        wait_all(send_sem.at[0, c], t_buf, c, 16)
        wait_all(send_sem.at[1, c], v_buf, c, 32)
        wait_all(send_sem.at[2, c], o_buf, c, 32)
        wait_all(send_sem.at[3, c], j_buf, c, 16)
    scope("wait_z_out3", wait_all, recv_sem.at[3, 3], s_buf, 3, 16)
    scope("last_rows", last_rows)


def per_device(mix_input, group_maps, out_map):
    tab = tables()
    names = ("chan", "in_flip", "dft", "turn", "last", "out_flip", "pick")
    arrays = [mix_input] + [jnp.asarray(tab[name]) for name in names] + [group_maps, out_map]
    hbm = pl.BlockSpec(memory_space=pltpu.HBM)
    model = out_map.shape[1]
    rows, part, late_map = pl.pallas_call(
        mix_kernel,
        out_shape=[jax.ShapeDtypeStruct(shape, BF16) for shape in ((512, 128), (512, model), (128, model))],
        in_specs=[hbm] * len(arrays),
        out_specs=[pl.BlockSpec(memory_space=pltpu.VMEM)] * 3,
        scratch_shapes=[pltpu.VMEM(a.shape, a.dtype) for a in arrays]
        + [
            pltpu.VMEM((4, 16, 32, 128), BF16),
            pltpu.VMEM((4, 16, 32, 128), BF16),
            pltpu.VMEM((4, 32, 16, 128), BF16),
            pltpu.VMEM((4, 32, 16, 128), BF16),
            pltpu.VMEM((1024, 128), F32),
            pltpu.VMEM((512, 256), BF16),
            pltpu.VMEM((4, 32, 2, 8, 128), BF16),
            pltpu.VMEM((4, 32, 2, 8, 128), BF16),
            pltpu.VMEM((4, 16, 32, 128), BF16),
            pltpu.VMEM((4, 16, 32, 128), BF16),
            pltpu.VMEM((3, 128, model), BF16),
            pltpu.VMEM((512, model), F32),
            pltpu.SemaphoreType.DMA((13,)),
            pltpu.SemaphoreType.DMA((4, 4)),
            pltpu.SemaphoreType.DMA((4, 4)),
        ],
        compiler_params=pltpu.CompilerParams(collective_id=0, has_side_effects=True, vmem_limit_bytes=40 * 2**20),
    )(*[pltpu.with_memory_space_constraint(a, pltpu.HBM) for a in arrays])
    mixed = jnp.dot(rows, late_map, preferred_element_type=F32) + part.astype(F32)
    return mixed.astype(BF16).reshape(4, 128, model)


def solution(mesh):
    return jax.shard_map(
        per_device,
        mesh=mesh,
        in_specs=(P(None, ("row", "col"), None), P(), P()),
        out_specs=P(None, ("row", "col"), None),
        check_vma=False,
    )
```

```python
import functools
import math

import jax
import jax.numpy as jnp
import numpy as np
from jax import lax
from jax.experimental import pallas as pl
from jax.experimental.pallas import tpu as pltpu
from jax.sharding import PartitionSpec as P

MESH = pl.DeviceIdType.MESH
F32, BF16 = jnp.float32, jnp.bfloat16
LENGTH, WIDTH = 65536, 128
SIDE = 4
HOPS = (0, 1, 2, 1)
RC_FAR_FIRST = tuple(
    sorted(
        ((dy, dx, dh) for dy in range(SIDE) for dx in range(SIDE) for dh in range(2) if dy or dx or dh),
        key=lambda step: (-HOPS[step[0]] - HOPS[step[1]], step[2], step),
    )
)
FAR_FIRST = (8, 7, 9, 6, 10, 5, 11, 4, 12, 3, 13, 2, 14, 1, 15)


@functools.cache
def tables():
    ch = np.arange(128)
    chan = np.zeros((2, 2, 32, 128))
    pick = np.zeros((2, 2, 32, 128))
    for c in range(2):
        for lg in range(32):
            l = 32 * c + lg
            chan[c, 0, lg] = np.cos(2 * np.pi * ((ch * l) % 128) / 128)
            chan[c, 1, lg] = -np.sin(2 * np.pi * ((ch * l) % 128) / 128) if l else np.cos(np.pi * ch)
            if l:
                pick[c, 0, lg, [l, 128 - l]] = 1, 1
                pick[c, 1, lg, [l, 128 - l]] = -1, 1
            else:
                pick[c, 0, lg, 0] = pick[c, 1, lg, 64] = 1
    in_flip = np.zeros((16, 16, 16, 16))
    out_flip = np.zeros((8, 32, 32, 8))
    for i in range(16):
        for j in range(16):
            in_flip[i, j, j, i] = 1
    for i in range(8):
        for j in range(32):
            out_flip[i, j, j, i] = 1
    src = np.arange(512)
    q = 32 * (src // 32) + src // 16 % 2 + 2 * (src % 16)
    k1 = np.arange(512)
    ang = 2 * np.pi * ((k1[:, None] * q[None, :]) % 512) / 512
    turn = 2 * np.pi * k1[:, None] * np.arange(128)[None, :] / LENGTH
    fang = 2 * np.pi * ((np.arange(128)[:, None] * np.arange(128)[None, :]) % 128) / 128
    last = np.stack(
        [np.concatenate([np.cos(fang), np.sin(fang)], axis=1), np.concatenate([-np.sin(fang), np.cos(fang)], axis=1)]
    ) / math.sqrt(LENGTH * WIDTH)
    return {
        "chan": chan.reshape(128, 128).astype(BF16),
        "in_flip": in_flip.reshape(256, 256).astype(BF16),
        "dft": np.concatenate([np.cos(ang), -np.sin(ang)]).astype(BF16),
        "turn": np.stack([np.cos(turn), np.sin(turn)]).astype(np.float32),
        "last": last.astype(BF16),
        "out_flip": out_flip.reshape(256, 256).astype(BF16),
        "pick": pick.reshape(128, 128).astype(BF16),
    }


def mix_kernel(
    x_hbm, chan_hbm, in_flip_hbm, dft_hbm, turn_hbm, last_hbm, out_flip_hbm, pick_hbm, group_hbm, out_map_hbm,
    rows_ref, part_ref, late_map_ref, x_ref, chan_ref, in_flip_ref, dft_ref, turn_ref, last_ref, out_flip_ref, pick_ref, group_ref, out_map_ref,
    t_buf, w_buf, v_buf, r_buf, f_buf, g_buf, o_buf, m_buf, j_buf, s_buf, fused_buf, acc_buf, load_sem, send_sem, recv_sem,
):
    row = lax.axis_index("row")
    col = lax.axis_index("col")
    z = col // 2
    h = col % 2
    me = 2 * row + h

    pairs = tuple((x_hbm.at[s], x_ref.at[s]) for s in range(4)) + (
        (chan_hbm, chan_ref), (in_flip_hbm, in_flip_ref), (dft_hbm, dft_ref), (turn_hbm, turn_ref),
        (last_hbm, last_ref), (out_flip_hbm, out_flip_ref), (pick_hbm, pick_ref), (group_hbm, group_ref),
        (out_map_hbm, out_map_ref),
    )
    loads = [pltpu.make_async_copy(src, dst, load_sem.at[i]) for i, (src, dst) in enumerate(pairs)]

    def rc_peer(step):
        dy, dx, dh = step
        peer_row = SIDE * lax.rem(row // SIDE + dy, SIDE) + lax.rem(row % SIDE + dx, SIDE)
        peer_core = lax.rem(h + dh, 2)
        return 2 * peer_row + peer_core, (peer_row, 2 * z + peer_core)

    def z_peer(step):
        peer = lax.rem(z + step, 16)
        return peer, (row, 2 * peer + h)

    barrier = pltpu.get_barrier_semaphore()

    for step in FAR_FIRST:
        pl.semaphore_signal(barrier, inc=1, device_id=z_peer(step)[1], device_id_type=MESH)
    for load in loads[:6]:
        load.start()
    for step in RC_FAR_FIRST:
        pl.semaphore_signal(barrier, inc=1, device_id=rc_peer(step)[1], device_id_type=MESH)

    def exchange(phase, c, src, dst, peer_of, slot, order, part=None):
        for step in order:
            peer, device = peer_of(step)
            send, land = src.at[c, peer], dst.at[c, slot]
            if part is not None:
                send, land = src.at[c, peer, pl.ds(16 * part, 16)], dst.at[c, slot, pl.ds(16 * part, 16)]
            pltpu.make_async_remote_copy(
                src_ref=send, dst_ref=land, send_sem=send_sem.at[phase, c], recv_sem=recv_sem.at[phase, c],
                device_id=device, device_id_type=MESH,
            ).start()
        if part != 1:
            dst[c, slot] = src[c, slot]

    def wait_all(sem, buf, c, count):
        span = buf.at[c, pl.ds(0, count - 1)]
        pltpu.make_async_copy(span, span, sem).wait()

    def channel_transform():
        for g in range(4):
            rhs = jnp.concatenate([x_ref[s, :, 128 * g : 128 * g + 128] for s in range(4)], axis=0)
            res = lax.dot_general(chan_ref[...], rhs, (((1,), (1,)), ((), ())), preferred_element_type=F32)
            res = res.astype(BF16)
            for c in range(4):
                for s in range(4):
                    t_buf[c, 4 * s + g] = res[32 * c : 32 * c + 32, 128 * s : 128 * s + 128]

    def turn(src, dst, c):
        rhs = jnp.concatenate([src[c, :, 16 * b : 16 * b + 16, :].reshape(256, 128) for b in range(2)], axis=1)
        res = jnp.dot(in_flip_ref[...], rhs, preferred_element_type=F32).astype(BF16)
        for b in range(2):
            for i in range(16):
                dst[c, 16 * b + i] = res[16 * i : 16 * i + 16, 128 * b : 128 * b + 128]

    def turn_back(src, dst, c):
        rhs = jnp.concatenate([src[c, 16 * b : 16 * b + 16].reshape(256, 128) for b in range(2)], axis=1)
        res = jnp.dot(in_flip_ref[...], rhs, preferred_element_type=F32).astype(BF16)
        for b in range(2):
            for i in range(16):
                dst[c, i, 16 * b : 16 * b + 16] = res[16 * i : 16 * i + 16, 128 * b : 128 * b + 128]

    def transform(c):
        f_buf[...] = jnp.dot(dft_ref[...], r_buf[c].reshape(512, 128), preferred_element_type=F32)

        def body(step, carry):
            rows = pl.ds(pl.multiple_of(64 * step, 64), 64)
            under = pl.ds(pl.multiple_of(512 + 64 * step, 64), 64)
            re, im, cos, sin = f_buf[rows, :], f_buf[under, :], turn_ref[0, rows, :], turn_ref[1, rows, :]
            g_buf[rows, 0:128] = (re * cos + im * sin).astype(BF16)
            g_buf[rows, 128:256] = (im * cos - re * sin).astype(BF16)
            return carry

        lax.fori_loop(0, 8, body, 0)
        kind = jnp.where(me == 0, 0, 1) if c == 1 else c % 2
        res = lax.dot_general(
            last_ref[kind], g_buf[...], (((1,), (1,)), ((), ())), preferred_element_type=F32
        ).astype(BF16)
        for fh in range(16):
            for e3 in range(2):
                for e4 in range(2):
                    at = 256 * e4 + 128 * e3
                    o_buf[c, 2 * fh + e3, e4] = res[8 * fh : 8 * fh + 8, at : at + 128]

    def out_turn(c):
        rhs = jnp.concatenate([m_buf[c, :, e4].reshape(256, 128) for e4 in range(2)], axis=1)
        res = jnp.dot(out_flip_ref[...], rhs, preferred_element_type=F32).astype(BF16)
        for fl in range(8):
            for e4 in range(2):
                j_buf[c, 2 * fl + e4] = res[32 * fl : 32 * fl + 32, 128 * e4 : 128 * e4 + 128]

    def fuse_maps():
        for g in range(4):
            chosen = jnp.dot(pick_ref[...], group_ref[g], preferred_element_type=F32).astype(BF16)
            for n in range(4):
                at = pl.ds(512 * n, 512)
                res = jnp.dot(chosen, out_map_ref[128 * g : 128 * g + 128, at], preferred_element_type=F32).astype(BF16)
                for c in range(3):
                    fused_buf[c, 32 * g : 32 * g + 32, at] = res[32 * c : 32 * c + 32]
                late_map_ref[32 * g : 32 * g + 32, at] = res[96:128]

    def spectrum_rows(c):
        return jnp.concatenate([s_buf[c, 4 * s : 4 * s + 4].reshape(128, 128).T for s in range(4)], axis=0)

    def first_product():
        lhs = jnp.concatenate([spectrum_rows(0), spectrum_rows(1)], axis=1)

        def body(n, carry):
            at = pl.ds(pl.multiple_of(256 * n, 256), 256)
            acc_buf[:, at] = jnp.dot(lhs, fused_buf[0:2, :, at].reshape(256, 256), preferred_element_type=F32)
            return carry

        lax.fori_loop(0, 8, body, 0)

    def second_product():
        lhs = spectrum_rows(2)

        def body(n, carry):
            at = pl.ds(pl.multiple_of(256 * n, 256), 256)
            res = jnp.dot(lhs, fused_buf[2, :, at], preferred_element_type=F32)
            part_ref[:, at] = (acc_buf[:, at] + res).astype(BF16)
            return carry

        lax.fori_loop(0, 8, body, 0)

    def last_rows():
        rows_ref[...] = spectrum_rows(3)

    def scope(name, run, *args):
        with jax.named_scope(name):
            run(*args)

    for load in loads[:6]:
        load.wait()
    scope("channel", channel_transform)
    scope("turn_x", turn, t_buf, v_buf, 0)
    with jax.named_scope("barrier"):
        pl.semaphore_wait(barrier, 46)
    exchange(1, 0, v_buf, r_buf, rc_peer, me, RC_FAR_FIRST)
    exchange(0, 1, t_buf, w_buf, z_peer, z, FAR_FIRST)
    for load in loads[6:]:
        load.start()
    for load in loads[6:]:
        load.wait()
    scope("fuse_maps", fuse_maps)

    def first_rc_in(c):
        scope(f"wait_rc_in{c}", wait_all, recv_sem.at[1, c], r_buf, c, 32)
        scope(f"turn_y{c}", turn_back, r_buf, t_buf, c)
        exchange(0, 0, t_buf, w_buf, z_peer, z, FAR_FIRST)
        exchange(0, 2, t_buf, w_buf, z_peer, z, FAR_FIRST)

    def first_z_in(c):
        scope(f"wait_z_in{c}", wait_all, recv_sem.at[0, c], w_buf, c, 16)
        scope(f"turn_z{c}", turn, w_buf, r_buf, c)
        scope(f"transform{c}", transform, c)
        exchange(2, c, o_buf, m_buf, rc_peer, me, RC_FAR_FIRST)

    def z_in(c):
        scope(f"wait_z_in{c}", wait_all, recv_sem.at[0, c], w_buf, c, 16)
        scope(f"in_turn{c}", turn, w_buf, v_buf, c)
        if c == 1:
            exchange(0, 3, t_buf, w_buf, z_peer, z, FAR_FIRST)
        exchange(1, c, v_buf, r_buf, rc_peer, me, RC_FAR_FIRST)

    def rc_in(c):
        scope(f"wait_rc_in{c}", wait_all, recv_sem.at[1, c], r_buf, c, 32)
        scope(f"transform{c}", transform, c)
        exchange(2, c, o_buf, m_buf, rc_peer, me, RC_FAR_FIRST)

    def rc_out(c):
        scope(f"wait_rc_out{c}", wait_all, recv_sem.at[2, c], m_buf, c, 32)
        scope(f"out_turn{c}", out_turn, c)
        exchange(3, c, j_buf, s_buf, z_peer, z, FAR_FIRST)

    order = (
        (first_rc_in, 0), (z_in, 1), (first_z_in, 0), (rc_in, 1), (z_in, 2), (rc_out, 0), (z_in, 3), (rc_out, 1),
        (rc_in, 2), (rc_in, 3), (rc_out, 2), (rc_out, 3),
    )
    for stage, c in order:
        stage(c)
    for c in range(2):
        scope(f"wait_z_out{c}", wait_all, recv_sem.at[3, c], s_buf, c, 16)
    scope("first_product", first_product)
    scope("wait_z_out2", wait_all, recv_sem.at[3, 2], s_buf, 2, 16)
    scope("second_product", second_product)
    for c in range(4):
        wait_all(send_sem.at[0, c], t_buf, c, 16)
        wait_all(send_sem.at[1, c], v_buf, c, 32)
        wait_all(send_sem.at[2, c], o_buf, c, 32)
        wait_all(send_sem.at[3, c], j_buf, c, 16)
    scope("wait_z_out3", wait_all, recv_sem.at[3, 3], s_buf, 3, 16)
    scope("last_rows", last_rows)


def per_device(mix_input, group_maps, out_map):
    tab = tables()
    names = ("chan", "in_flip", "dft", "turn", "last", "out_flip", "pick")
    arrays = [mix_input] + [jnp.asarray(tab[name]) for name in names] + [group_maps, out_map]
    hbm = pl.BlockSpec(memory_space=pltpu.HBM)
    model = out_map.shape[1]
    rows, part, late_map = pl.pallas_call(
        mix_kernel,
        out_shape=[jax.ShapeDtypeStruct(shape, BF16) for shape in ((512, 128), (512, model), (128, model))],
        in_specs=[hbm] * len(arrays),
        out_specs=[pl.BlockSpec(memory_space=pltpu.VMEM)] * 3,
        scratch_shapes=[pltpu.VMEM(a.shape, a.dtype) for a in arrays]
        + [
            pltpu.VMEM((4, 16, 32, 128), BF16),
            pltpu.VMEM((4, 16, 32, 128), BF16),
            pltpu.VMEM((4, 32, 16, 128), BF16),
            pltpu.VMEM((4, 32, 16, 128), BF16),
            pltpu.VMEM((1024, 128), F32),
            pltpu.VMEM((512, 256), BF16),
            pltpu.VMEM((4, 32, 2, 8, 128), BF16),
            pltpu.VMEM((4, 32, 2, 8, 128), BF16),
            pltpu.VMEM((4, 16, 32, 128), BF16),
            pltpu.VMEM((4, 16, 32, 128), BF16),
            pltpu.VMEM((3, 128, model), BF16),
            pltpu.VMEM((512, model), F32),
            pltpu.SemaphoreType.DMA((13,)),
            pltpu.SemaphoreType.DMA((4, 4)),
            pltpu.SemaphoreType.DMA((4, 4)),
        ],
        compiler_params=pltpu.CompilerParams(collective_id=0, has_side_effects=True, vmem_limit_bytes=40 * 2**20),
    )(*[pltpu.with_memory_space_constraint(a, pltpu.HBM) for a in arrays])
    mixed = jnp.dot(rows, late_map, preferred_element_type=F32) + part.astype(F32)
    return mixed.astype(BF16).reshape(4, 128, model)


def solution(mesh):
    return jax.shard_map(
        per_device,
        mesh=mesh,
        in_specs=(P(None, ("row", "col"), None), P(), P()),
        out_specs=P(None, ("row", "col"), None),
        check_vma=False,
    )
```

```python
import functools
import math

import jax
import jax.numpy as jnp
import numpy as np
from jax import lax
from jax.experimental import pallas as pl
from jax.experimental.pallas import tpu as pltpu
from jax.sharding import PartitionSpec as P

MESH = pl.DeviceIdType.MESH
F32, BF16 = jnp.float32, jnp.bfloat16
LENGTH, WIDTH = 65536, 128
SIDE = 4
HOPS = (0, 1, 2, 1)
RC_FAR_FIRST = tuple(
    sorted(
        ((dy, dx, dh) for dy in range(SIDE) for dx in range(SIDE) for dh in range(2) if dy or dx or dh),
        key=lambda step: (-HOPS[step[0]] - HOPS[step[1]], step[2], step),
    )
)
FAR_FIRST = (8, 7, 9, 6, 10, 5, 11, 4, 12, 3, 13, 2, 14, 1, 15)


@functools.cache
def tables():
    ch = np.arange(128)
    chan = np.zeros((2, 2, 32, 128))
    pick = np.zeros((2, 2, 32, 128))
    for c in range(2):
        for lg in range(32):
            l = 32 * c + lg
            chan[c, 0, lg] = np.cos(2 * np.pi * ((ch * l) % 128) / 128)
            chan[c, 1, lg] = -np.sin(2 * np.pi * ((ch * l) % 128) / 128) if l else np.cos(np.pi * ch)
            if l:
                pick[c, 0, lg, [l, 128 - l]] = 1, 1
                pick[c, 1, lg, [l, 128 - l]] = -1, 1
            else:
                pick[c, 0, lg, 0] = pick[c, 1, lg, 64] = 1
    in_flip = np.zeros((16, 16, 16, 16))
    out_flip = np.zeros((8, 32, 32, 8))
    for i in range(16):
        for j in range(16):
            in_flip[i, j, j, i] = 1
    for i in range(8):
        for j in range(32):
            out_flip[i, j, j, i] = 1
    src = np.arange(512)
    q = 32 * (src // 32) + src // 16 % 2 + 2 * (src % 16)
    k1 = np.arange(512)
    ang = 2 * np.pi * ((k1[:, None] * q[None, :]) % 512) / 512
    turn = 2 * np.pi * k1[:, None] * np.arange(128)[None, :] / LENGTH
    fang = 2 * np.pi * ((np.arange(128)[:, None] * np.arange(128)[None, :]) % 128) / 128
    last = np.stack(
        [np.concatenate([np.cos(fang), np.sin(fang)], axis=1), np.concatenate([-np.sin(fang), np.cos(fang)], axis=1)]
    ) / math.sqrt(LENGTH * WIDTH)
    return {
        "chan": chan.reshape(128, 128).astype(BF16),
        "in_flip": in_flip.reshape(256, 256).astype(BF16),
        "dft": np.concatenate([np.cos(ang), -np.sin(ang)]).astype(BF16),
        "turn": np.stack([np.cos(turn), np.sin(turn)]).astype(np.float32),
        "last": last.astype(BF16),
        "out_flip": out_flip.reshape(256, 256).astype(BF16),
        "pick": pick.reshape(128, 128).astype(BF16),
    }


def mix_kernel(
    x_hbm, chan_hbm, in_flip_hbm, dft_hbm, turn_hbm, last_hbm, out_flip_hbm, pick_hbm, group_hbm, out_map_hbm,
    rows_ref, part_ref, late_map_ref, x_ref, chan_ref, in_flip_ref, dft_ref, turn_ref, last_ref, out_flip_ref, pick_ref, group_ref, out_map_ref,
    t_buf, w_buf, v_buf, r_buf, g_buf, o_buf, m_buf, j_buf, s_buf, fused_buf, acc_buf, load_sem, send_sem, recv_sem,
):
    row = lax.axis_index("row")
    col = lax.axis_index("col")
    z = col // 2
    h = col % 2
    me = 2 * row + h

    pairs = tuple((x_hbm.at[s], x_ref.at[s]) for s in range(4)) + (
        (chan_hbm, chan_ref), (in_flip_hbm, in_flip_ref), (dft_hbm, dft_ref), (turn_hbm, turn_ref),
        (last_hbm, last_ref), (out_flip_hbm, out_flip_ref), (pick_hbm, pick_ref), (group_hbm, group_ref),
        (out_map_hbm, out_map_ref),
    )
    loads = [pltpu.make_async_copy(src, dst, load_sem.at[i]) for i, (src, dst) in enumerate(pairs)]

    def rc_peer(step):
        dy, dx, dh = step
        peer_row = SIDE * lax.rem(row // SIDE + dy, SIDE) + lax.rem(row % SIDE + dx, SIDE)
        peer_core = lax.rem(h + dh, 2)
        return 2 * peer_row + peer_core, (peer_row, 2 * z + peer_core)

    def z_peer(step):
        peer = lax.rem(z + step, 16)
        return peer, (row, 2 * peer + h)

    barrier = pltpu.get_barrier_semaphore()

    for step in FAR_FIRST:
        pl.semaphore_signal(barrier, inc=1, device_id=z_peer(step)[1], device_id_type=MESH)
    for load in loads[:6]:
        load.start()
    for step in RC_FAR_FIRST:
        pl.semaphore_signal(barrier, inc=1, device_id=rc_peer(step)[1], device_id_type=MESH)

    def exchange(phase, c, src, dst, peer_of, slot, order, part=None):
        for step in order:
            peer, device = peer_of(step)
            send, land = src.at[c, peer], dst.at[c, slot]
            if part is not None:
                send, land = src.at[c, peer, pl.ds(16 * part, 16)], dst.at[c, slot, pl.ds(16 * part, 16)]
            pltpu.make_async_remote_copy(
                src_ref=send, dst_ref=land, send_sem=send_sem.at[phase, c], recv_sem=recv_sem.at[phase, c],
                device_id=device, device_id_type=MESH,
            ).start()
        if part != 1:
            dst[c, slot] = src[c, slot]

    def wait_all(sem, buf, c, count):
        span = buf.at[c, pl.ds(0, count - 1)]
        pltpu.make_async_copy(span, span, sem).wait()

    def channel_transform():
        for g in range(4):
            rhs = jnp.concatenate([x_ref[s, :, 128 * g : 128 * g + 128] for s in range(4)], axis=0)
            res = lax.dot_general(chan_ref[...], rhs, (((1,), (1,)), ((), ())), preferred_element_type=F32)
            res = res.astype(BF16)
            for c in range(4):
                for s in range(4):
                    t_buf[c, 4 * s + g] = res[32 * c : 32 * c + 32, 128 * s : 128 * s + 128]

    def turn(src, dst, c):
        rhs = jnp.concatenate([src[c, :, 16 * b : 16 * b + 16, :].reshape(256, 128) for b in range(2)], axis=1)
        res = jnp.dot(in_flip_ref[...], rhs, preferred_element_type=F32).astype(BF16)
        for b in range(2):
            for i in range(16):
                dst[c, 16 * b + i] = res[16 * i : 16 * i + 16, 128 * b : 128 * b + 128]

    def turn_back(src, dst, c):
        rhs = jnp.concatenate([src[c, 16 * b : 16 * b + 16].reshape(256, 128) for b in range(2)], axis=1)
        res = jnp.dot(in_flip_ref[...], rhs, preferred_element_type=F32).astype(BF16)
        for b in range(2):
            for i in range(16):
                dst[c, i, 16 * b : 16 * b + 16] = res[16 * i : 16 * i + 16, 128 * b : 128 * b + 128]

    def transform(c):
        rhs = r_buf[c].reshape(512, 128)

        for step in range(2):
            rows, under = pl.ds(256 * step, 256), pl.ds(512 + 256 * step, 256)
            re = jnp.dot(dft_ref[rows, :], rhs, preferred_element_type=F32)
            im = jnp.dot(dft_ref[under, :], rhs, preferred_element_type=F32)
            cos, sin = turn_ref[0, rows, :], turn_ref[1, rows, :]
            g_buf[rows, 0:128] = (re * cos + im * sin).astype(BF16)
            g_buf[rows, 128:256] = (im * cos - re * sin).astype(BF16)
        kind = jnp.where(me == 0, 0, 1) if c == 1 else c % 2
        res = lax.dot_general(
            last_ref[kind], g_buf[...], (((1,), (1,)), ((), ())), preferred_element_type=F32
        ).astype(BF16)
        for fh in range(16):
            for e3 in range(2):
                for e4 in range(2):
                    at = 256 * e4 + 128 * e3
                    o_buf[c, 2 * fh + e3, e4] = res[8 * fh : 8 * fh + 8, at : at + 128]

    def out_turn(c):
        rhs = jnp.concatenate([m_buf[c, :, e4].reshape(256, 128) for e4 in range(2)], axis=1)
        res = jnp.dot(out_flip_ref[...], rhs, preferred_element_type=F32).astype(BF16)
        for fl in range(8):
            for e4 in range(2):
                j_buf[c, 2 * fl + e4] = res[32 * fl : 32 * fl + 32, 128 * e4 : 128 * e4 + 128]

    def fuse_maps():
        for g in range(4):
            chosen = jnp.dot(pick_ref[...], group_ref[g], preferred_element_type=F32).astype(BF16)
            for n in range(4):
                at = pl.ds(512 * n, 512)
                res = jnp.dot(chosen, out_map_ref[128 * g : 128 * g + 128, at], preferred_element_type=F32).astype(BF16)
                for c in range(3):
                    fused_buf[c, 32 * g : 32 * g + 32, at] = res[32 * c : 32 * c + 32]
                late_map_ref[32 * g : 32 * g + 32, at] = res[96:128]

    def spectrum_rows(c):
        return jnp.concatenate([s_buf[c, 4 * s : 4 * s + 4].reshape(128, 128).T for s in range(4)], axis=0)

    def first_product():
        lhs = jnp.concatenate([spectrum_rows(0), spectrum_rows(1)], axis=1)

        def body(n, carry):
            at = pl.ds(pl.multiple_of(256 * n, 256), 256)
            acc_buf[:, at] = jnp.dot(lhs, fused_buf[0:2, :, at].reshape(256, 256), preferred_element_type=F32)
            return carry

        lax.fori_loop(0, 8, body, 0)

    def second_product():
        lhs = spectrum_rows(2)

        def body(n, carry):
            at = pl.ds(pl.multiple_of(256 * n, 256), 256)
            res = jnp.dot(lhs, fused_buf[2, :, at], preferred_element_type=F32)
            part_ref[:, at] = (acc_buf[:, at] + res).astype(BF16)
            return carry

        lax.fori_loop(0, 8, body, 0)

    def last_rows():
        rows_ref[...] = spectrum_rows(3)

    def scope(name, run, *args):
        with jax.named_scope(name):
            run(*args)

    for load in loads[:6]:
        load.wait()
    scope("channel", channel_transform)
    scope("turn_x", turn, t_buf, v_buf, 0)
    with jax.named_scope("barrier"):
        pl.semaphore_wait(barrier, 46)
    exchange(1, 0, v_buf, r_buf, rc_peer, me, RC_FAR_FIRST)
    exchange(0, 1, t_buf, w_buf, z_peer, z, FAR_FIRST)
    for load in loads[6:]:
        load.start()
    for load in loads[6:]:
        load.wait()
    scope("fuse_maps", fuse_maps)

    def first_rc_in(c):
        scope(f"wait_rc_in{c}", wait_all, recv_sem.at[1, c], r_buf, c, 32)
        scope(f"turn_y{c}", turn_back, r_buf, t_buf, c)
        exchange(0, 0, t_buf, w_buf, z_peer, z, FAR_FIRST)
        exchange(0, 2, t_buf, w_buf, z_peer, z, FAR_FIRST)

    def first_z_in(c):
        scope(f"wait_z_in{c}", wait_all, recv_sem.at[0, c], w_buf, c, 16)
        scope(f"turn_z{c}", turn, w_buf, r_buf, c)
        scope(f"transform{c}", transform, c)
        exchange(2, c, o_buf, m_buf, rc_peer, me, RC_FAR_FIRST)

    def z_in(c):
        scope(f"wait_z_in{c}", wait_all, recv_sem.at[0, c], w_buf, c, 16)
        scope(f"in_turn{c}", turn, w_buf, v_buf, c)
        if c == 1:
            exchange(0, 3, t_buf, w_buf, z_peer, z, FAR_FIRST)
        exchange(1, c, v_buf, r_buf, rc_peer, me, RC_FAR_FIRST)

    def rc_in(c):
        scope(f"wait_rc_in{c}", wait_all, recv_sem.at[1, c], r_buf, c, 32)
        scope(f"transform{c}", transform, c)
        exchange(2, c, o_buf, m_buf, rc_peer, me, RC_FAR_FIRST)

    def rc_out(c):
        scope(f"wait_rc_out{c}", wait_all, recv_sem.at[2, c], m_buf, c, 32)
        scope(f"out_turn{c}", out_turn, c)
        exchange(3, c, j_buf, s_buf, z_peer, z, FAR_FIRST)

    order = (
        (first_rc_in, 0), (z_in, 1), (first_z_in, 0), (rc_in, 1), (z_in, 2), (rc_out, 0), (z_in, 3), (rc_out, 1),
        (rc_in, 2), (rc_in, 3), (rc_out, 2), (rc_out, 3),
    )
    for stage, c in order:
        stage(c)
    for c in range(2):
        scope(f"wait_z_out{c}", wait_all, recv_sem.at[3, c], s_buf, c, 16)
    scope("first_product", first_product)
    scope("wait_z_out2", wait_all, recv_sem.at[3, 2], s_buf, 2, 16)
    scope("second_product", second_product)
    for c in range(4):
        wait_all(send_sem.at[0, c], t_buf, c, 16)
        wait_all(send_sem.at[1, c], v_buf, c, 32)
        wait_all(send_sem.at[2, c], o_buf, c, 32)
        wait_all(send_sem.at[3, c], j_buf, c, 16)
    scope("wait_z_out3", wait_all, recv_sem.at[3, 3], s_buf, 3, 16)
    scope("last_rows", last_rows)


def per_device(mix_input, group_maps, out_map):
    tab = tables()
    names = ("chan", "in_flip", "dft", "turn", "last", "out_flip", "pick")
    arrays = [mix_input] + [jnp.asarray(tab[name]) for name in names] + [group_maps, out_map]
    hbm = pl.BlockSpec(memory_space=pltpu.HBM)
    model = out_map.shape[1]
    rows, part, late_map = pl.pallas_call(
        mix_kernel,
        out_shape=[jax.ShapeDtypeStruct(shape, BF16) for shape in ((512, 128), (512, model), (128, model))],
        in_specs=[hbm] * len(arrays),
        out_specs=[pl.BlockSpec(memory_space=pltpu.VMEM)] * 3,
        scratch_shapes=[pltpu.VMEM(a.shape, a.dtype) for a in arrays]
        + [
            pltpu.VMEM((4, 16, 32, 128), BF16),
            pltpu.VMEM((4, 16, 32, 128), BF16),
            pltpu.VMEM((4, 32, 16, 128), BF16),
            pltpu.VMEM((4, 32, 16, 128), BF16),
            pltpu.VMEM((512, 256), BF16),
            pltpu.VMEM((4, 32, 2, 8, 128), BF16),
            pltpu.VMEM((4, 32, 2, 8, 128), BF16),
            pltpu.VMEM((4, 16, 32, 128), BF16),
            pltpu.VMEM((4, 16, 32, 128), BF16),
            pltpu.VMEM((3, 128, model), BF16),
            pltpu.VMEM((512, model), F32),
            pltpu.SemaphoreType.DMA((13,)),
            pltpu.SemaphoreType.DMA((4, 4)),
            pltpu.SemaphoreType.DMA((4, 4)),
        ],
        compiler_params=pltpu.CompilerParams(collective_id=0, has_side_effects=True, vmem_limit_bytes=40 * 2**20),
    )(*[pltpu.with_memory_space_constraint(a, pltpu.HBM) for a in arrays])
    mixed = jnp.dot(rows, late_map, preferred_element_type=F32) + part.astype(F32)
    return mixed.astype(BF16).reshape(4, 128, model)


def solution(mesh):
    return jax.shard_map(
        per_device,
        mesh=mesh,
        in_specs=(P(None, ("row", "col"), None), P(), P()),
        out_specs=P(None, ("row", "col"), None),
        check_vma=False,
    )
```

```python
import functools
import math

import jax
import jax.numpy as jnp
import numpy as np
from jax import lax
from jax.experimental import pallas as pl
from jax.experimental.pallas import tpu as pltpu
from jax.sharding import PartitionSpec as P

MESH = pl.DeviceIdType.MESH
F32, BF16 = jnp.float32, jnp.bfloat16
LENGTH, WIDTH = 65536, 128
SIDE = 4
HOPS = (0, 1, 2, 1)
RC_FAR_FIRST = tuple(
    sorted(
        ((dy, dx, dh) for dy in range(SIDE) for dx in range(SIDE) for dh in range(2) if dy or dx or dh),
        key=lambda step: (-HOPS[step[0]] - HOPS[step[1]], step[2], step),
    )
)
FAR_FIRST = (8, 7, 9, 6, 10, 5, 11, 4, 12, 3, 13, 2, 14, 1, 15)


@functools.cache
def tables():
    ch = np.arange(128)
    chan = np.zeros((2, 2, 32, 128))
    pick = np.zeros((2, 2, 32, 128))
    for c in range(2):
        for lg in range(32):
            l = 32 * c + lg
            chan[c, 0, lg] = np.cos(2 * np.pi * ((ch * l) % 128) / 128)
            chan[c, 1, lg] = -np.sin(2 * np.pi * ((ch * l) % 128) / 128) if l else np.cos(np.pi * ch)
            if l:
                pick[c, 0, lg, [l, 128 - l]] = 1, 1
                pick[c, 1, lg, [l, 128 - l]] = -1, 1
            else:
                pick[c, 0, lg, 0] = pick[c, 1, lg, 64] = 1
    in_flip = np.zeros((16, 16, 16, 16))
    out_flip = np.zeros((8, 32, 32, 8))
    for i in range(16):
        for j in range(16):
            in_flip[i, j, j, i] = 1
    for i in range(8):
        for j in range(32):
            out_flip[i, j, j, i] = 1
    src = np.arange(512)
    q = 32 * (src // 32) + src // 16 % 2 + 2 * (src % 16)
    k1 = np.arange(512)
    ang = 2 * np.pi * ((k1[:, None] * q[None, :]) % 512) / 512
    turn = 2 * np.pi * k1[:, None] * np.arange(128)[None, :] / LENGTH
    fang = 2 * np.pi * ((np.arange(128)[:, None] * np.arange(128)[None, :]) % 128) / 128
    last = np.stack(
        [np.concatenate([np.cos(fang), np.sin(fang)], axis=1), np.concatenate([-np.sin(fang), np.cos(fang)], axis=1)]
    ) / math.sqrt(LENGTH * WIDTH)
    return {
        "chan": chan.reshape(128, 128).astype(BF16),
        "in_flip": in_flip.reshape(256, 256).astype(BF16),
        "dft": np.concatenate([np.cos(ang), -np.sin(ang)]).astype(BF16),
        "turn": np.stack([np.cos(turn), np.sin(turn)]).astype(np.float32),
        "last": last.astype(BF16),
        "out_flip": out_flip.reshape(256, 256).astype(BF16),
        "pick": pick.reshape(128, 128).astype(BF16),
    }


def mix_kernel(
    x_hbm, chan_hbm, in_flip_hbm, dft_hbm, turn_hbm, last_hbm, out_flip_hbm, pick_hbm, group_hbm, out_map_hbm,
    rows_ref, part_ref, late_map_ref, x_ref, chan_ref, in_flip_ref, dft_ref, turn_ref, last_ref, out_flip_ref, pick_ref, group_ref, out_map_ref,
    t_buf, w_buf, v_buf, r_buf, g_buf, o_buf, m_buf, j_buf, s_buf, fused_buf, acc_buf, load_sem, send_sem, recv_sem,
):
    row = lax.axis_index("row")
    col = lax.axis_index("col")
    z = col // 2
    h = col % 2
    me = 2 * row + h

    pairs = tuple((x_hbm.at[s], x_ref.at[s]) for s in range(4)) + (
        (chan_hbm, chan_ref), (in_flip_hbm, in_flip_ref), (dft_hbm, dft_ref), (turn_hbm, turn_ref),
        (last_hbm, last_ref), (out_flip_hbm, out_flip_ref), (pick_hbm, pick_ref), (group_hbm, group_ref),
        (out_map_hbm, out_map_ref),
    )
    loads = [pltpu.make_async_copy(src, dst, load_sem.at[i]) for i, (src, dst) in enumerate(pairs)]

    def rc_peer(step):
        dy, dx, dh = step
        peer_row = SIDE * lax.rem(row // SIDE + dy, SIDE) + lax.rem(row % SIDE + dx, SIDE)
        peer_core = lax.rem(h + dh, 2)
        return 2 * peer_row + peer_core, (peer_row, 2 * z + peer_core)

    def z_peer(step):
        peer = lax.rem(z + step, 16)
        return peer, (row, 2 * peer + h)

    barrier = pltpu.get_barrier_semaphore()

    def greet(peer_of, steps):
        for step in steps:
            pl.semaphore_signal(barrier, inc=1, device_id=peer_of(step)[1], device_id_type=MESH)

    greet(z_peer, FAR_FIRST[:9])
    greet(rc_peer, RC_FAR_FIRST[:10])
    for load in loads[:6]:
        load.start()
    greet(z_peer, FAR_FIRST[9:])
    greet(rc_peer, RC_FAR_FIRST[10:])

    def exchange(phase, c, src, dst, peer_of, slot, order, part=None):
        for step in order:
            peer, device = peer_of(step)
            send, land = src.at[c, peer], dst.at[c, slot]
            if part is not None:
                send, land = src.at[c, peer, pl.ds(16 * part, 16)], dst.at[c, slot, pl.ds(16 * part, 16)]
            pltpu.make_async_remote_copy(
                src_ref=send, dst_ref=land, send_sem=send_sem.at[phase, c], recv_sem=recv_sem.at[phase, c],
                device_id=device, device_id_type=MESH,
            ).start()
        if part != 1:
            dst[c, slot] = src[c, slot]

    def wait_all(sem, buf, c, count):
        span = buf.at[c, pl.ds(0, count - 1)]
        pltpu.make_async_copy(span, span, sem).wait()

    def channel_transform():
        for g in range(4):
            rhs = jnp.concatenate([x_ref[s, :, 128 * g : 128 * g + 128] for s in range(4)], axis=0)
            res = lax.dot_general(chan_ref[...], rhs, (((1,), (1,)), ((), ())), preferred_element_type=F32)
            res = res.astype(BF16)
            for c in range(4):
                for s in range(4):
                    t_buf[c, 4 * s + g] = res[32 * c : 32 * c + 32, 128 * s : 128 * s + 128]

    def turn(src, dst, c):
        rhs = jnp.concatenate([src[c, :, 16 * b : 16 * b + 16, :].reshape(256, 128) for b in range(2)], axis=1)
        res = jnp.dot(in_flip_ref[...], rhs, preferred_element_type=F32).astype(BF16)
        for b in range(2):
            for i in range(16):
                dst[c, 16 * b + i] = res[16 * i : 16 * i + 16, 128 * b : 128 * b + 128]

    def turn_back(src, dst, c):
        rhs = jnp.concatenate([src[c, 16 * b : 16 * b + 16].reshape(256, 128) for b in range(2)], axis=1)
        res = jnp.dot(in_flip_ref[...], rhs, preferred_element_type=F32).astype(BF16)
        for b in range(2):
            for i in range(16):
                dst[c, i, 16 * b : 16 * b + 16] = res[16 * i : 16 * i + 16, 128 * b : 128 * b + 128]

    def transform(c):
        rhs = r_buf[c].reshape(512, 128)

        for step in range(2):
            rows, under = pl.ds(256 * step, 256), pl.ds(512 + 256 * step, 256)
            re = jnp.dot(dft_ref[rows, :], rhs, preferred_element_type=F32)
            im = jnp.dot(dft_ref[under, :], rhs, preferred_element_type=F32)
            cos, sin = turn_ref[0, rows, :], turn_ref[1, rows, :]
            g_buf[rows, 0:128] = (re * cos + im * sin).astype(BF16)
            g_buf[rows, 128:256] = (im * cos - re * sin).astype(BF16)
        kind = jnp.where(me == 0, 0, 1) if c == 1 else c % 2
        res = lax.dot_general(
            last_ref[kind], g_buf[...], (((1,), (1,)), ((), ())), preferred_element_type=F32
        ).astype(BF16)
        for fh in range(16):
            for e3 in range(2):
                for e4 in range(2):
                    at = 256 * e4 + 128 * e3
                    o_buf[c, 2 * fh + e3, e4] = res[8 * fh : 8 * fh + 8, at : at + 128]

    def out_turn(c):
        rhs = jnp.concatenate([m_buf[c, :, e4].reshape(256, 128) for e4 in range(2)], axis=1)
        res = jnp.dot(out_flip_ref[...], rhs, preferred_element_type=F32).astype(BF16)
        for fl in range(8):
            for e4 in range(2):
                j_buf[c, 2 * fl + e4] = res[32 * fl : 32 * fl + 32, 128 * e4 : 128 * e4 + 128]

    def fuse_maps():
        for g in range(4):
            chosen = jnp.dot(pick_ref[...], group_ref[g], preferred_element_type=F32).astype(BF16)
            for n in range(4):
                at = pl.ds(512 * n, 512)
                res = jnp.dot(chosen, out_map_ref[128 * g : 128 * g + 128, at], preferred_element_type=F32).astype(BF16)
                for c in range(3):
                    fused_buf[c, 32 * g : 32 * g + 32, at] = res[32 * c : 32 * c + 32]
                late_map_ref[32 * g : 32 * g + 32, at] = res[96:128]

    def spectrum_rows(c):
        return jnp.concatenate([s_buf[c, 4 * s : 4 * s + 4].reshape(128, 128).T for s in range(4)], axis=0)

    def first_product():
        lhs = jnp.concatenate([spectrum_rows(0), spectrum_rows(1)], axis=1)

        def body(n, carry):
            at = pl.ds(pl.multiple_of(256 * n, 256), 256)
            acc_buf[:, at] = jnp.dot(lhs, fused_buf[0:2, :, at].reshape(256, 256), preferred_element_type=F32)
            return carry

        lax.fori_loop(0, 8, body, 0)

    def second_product():
        lhs = spectrum_rows(2)

        def body(n, carry):
            at = pl.ds(pl.multiple_of(256 * n, 256), 256)
            res = jnp.dot(lhs, fused_buf[2, :, at], preferred_element_type=F32)
            part_ref[:, at] = (acc_buf[:, at] + res).astype(BF16)
            return carry

        lax.fori_loop(0, 8, body, 0)

    def last_rows():
        rows_ref[...] = spectrum_rows(3)

    def scope(name, run, *args):
        with jax.named_scope(name):
            run(*args)

    for load in loads[:6]:
        load.wait()
    scope("channel", channel_transform)
    scope("turn_x", turn, t_buf, v_buf, 0)
    with jax.named_scope("barrier"):
        pl.semaphore_wait(barrier, 46)
    exchange(1, 0, v_buf, r_buf, rc_peer, me, RC_FAR_FIRST)
    exchange(0, 1, t_buf, w_buf, z_peer, z, FAR_FIRST)
    for load in loads[6:]:
        load.start()
    for load in loads[6:]:
        load.wait()
    scope("fuse_maps", fuse_maps)

    def first_rc_in(c):
        scope(f"wait_rc_in{c}", wait_all, recv_sem.at[1, c], r_buf, c, 32)
        scope(f"turn_y{c}", turn_back, r_buf, t_buf, c)
        exchange(0, 0, t_buf, w_buf, z_peer, z, FAR_FIRST)
        exchange(0, 2, t_buf, w_buf, z_peer, z, FAR_FIRST)

    def first_z_in(c):
        scope(f"wait_z_in{c}", wait_all, recv_sem.at[0, c], w_buf, c, 16)
        scope(f"turn_z{c}", turn, w_buf, r_buf, c)
        scope(f"transform{c}", transform, c)
        exchange(2, c, o_buf, m_buf, rc_peer, me, RC_FAR_FIRST)

    def z_in(c):
        scope(f"wait_z_in{c}", wait_all, recv_sem.at[0, c], w_buf, c, 16)
        scope(f"in_turn{c}", turn, w_buf, v_buf, c)
        if c == 1:
            exchange(0, 3, t_buf, w_buf, z_peer, z, FAR_FIRST)
        exchange(1, c, v_buf, r_buf, rc_peer, me, RC_FAR_FIRST)

    def rc_in(c):
        scope(f"wait_rc_in{c}", wait_all, recv_sem.at[1, c], r_buf, c, 32)
        scope(f"transform{c}", transform, c)
        exchange(2, c, o_buf, m_buf, rc_peer, me, RC_FAR_FIRST)

    def rc_out(c):
        scope(f"wait_rc_out{c}", wait_all, recv_sem.at[2, c], m_buf, c, 32)
        scope(f"out_turn{c}", out_turn, c)
        exchange(3, c, j_buf, s_buf, z_peer, z, FAR_FIRST)

    order = (
        (first_rc_in, 0), (z_in, 1), (first_z_in, 0), (rc_in, 1), (z_in, 2), (rc_out, 0), (z_in, 3), (rc_out, 1),
        (rc_in, 2), (rc_in, 3), (rc_out, 2), (rc_out, 3),
    )
    for stage, c in order:
        stage(c)
    for c in range(2):
        scope(f"wait_z_out{c}", wait_all, recv_sem.at[3, c], s_buf, c, 16)
    scope("first_product", first_product)
    scope("wait_z_out2", wait_all, recv_sem.at[3, 2], s_buf, 2, 16)
    scope("second_product", second_product)
    for c in range(4):
        wait_all(send_sem.at[0, c], t_buf, c, 16)
        wait_all(send_sem.at[1, c], v_buf, c, 32)
        wait_all(send_sem.at[2, c], o_buf, c, 32)
        wait_all(send_sem.at[3, c], j_buf, c, 16)
    scope("wait_z_out3", wait_all, recv_sem.at[3, 3], s_buf, 3, 16)
    scope("last_rows", last_rows)


def per_device(mix_input, group_maps, out_map):
    tab = tables()
    names = ("chan", "in_flip", "dft", "turn", "last", "out_flip", "pick")
    arrays = [mix_input] + [jnp.asarray(tab[name]) for name in names] + [group_maps, out_map]
    hbm = pl.BlockSpec(memory_space=pltpu.HBM)
    model = out_map.shape[1]
    rows, part, late_map = pl.pallas_call(
        mix_kernel,
        out_shape=[jax.ShapeDtypeStruct(shape, BF16) for shape in ((512, 128), (512, model), (128, model))],
        in_specs=[hbm] * len(arrays),
        out_specs=[pl.BlockSpec(memory_space=pltpu.VMEM)] * 3,
        scratch_shapes=[pltpu.VMEM(a.shape, a.dtype) for a in arrays]
        + [
            pltpu.VMEM((4, 16, 32, 128), BF16),
            pltpu.VMEM((4, 16, 32, 128), BF16),
            pltpu.VMEM((4, 32, 16, 128), BF16),
            pltpu.VMEM((4, 32, 16, 128), BF16),
            pltpu.VMEM((512, 256), BF16),
            pltpu.VMEM((4, 32, 2, 8, 128), BF16),
            pltpu.VMEM((4, 32, 2, 8, 128), BF16),
            pltpu.VMEM((4, 16, 32, 128), BF16),
            pltpu.VMEM((4, 16, 32, 128), BF16),
            pltpu.VMEM((3, 128, model), BF16),
            pltpu.VMEM((512, model), F32),
            pltpu.SemaphoreType.DMA((13,)),
            pltpu.SemaphoreType.DMA((4, 4)),
            pltpu.SemaphoreType.DMA((4, 4)),
        ],
        compiler_params=pltpu.CompilerParams(collective_id=0, has_side_effects=True, vmem_limit_bytes=40 * 2**20),
    )(*[pltpu.with_memory_space_constraint(a, pltpu.HBM) for a in arrays])
    mixed = jnp.dot(rows, late_map, preferred_element_type=F32) + part.astype(F32)
    return mixed.astype(BF16).reshape(4, 128, model)


def solution(mesh):
    return jax.shard_map(
        per_device,
        mesh=mesh,
        in_specs=(P(None, ("row", "col"), None), P(), P()),
        out_specs=P(None, ("row", "col"), None),
        check_vma=False,
    )
```
